128 devices in a mesh: sp: 16 (over z, x), tp: 8 (over y, core).
Axes of the slice: x: 4, y: 4, z: 4, core: 2. Of those that a mesh axis runs over, the one named last changes fastest.
Arguments:
- queries: bfloat16 [16384, 1024], P('sp', 'tp'), may hold values from -75 to 75
- key_rows: bfloat16 [16384, 1024], P('sp', 'tp'), may hold values from -4 to 4
- value_rows: bfloat16 [16384, 1024], P('sp', 'tp'), may hold values from -6 to 6
- cum_gate: float32 [16, 16384], P('tp'), may hold values from -2342 to 0, as said below
- residual: bfloat16 [16384, 2048], P(('sp', 'tp')), may hold values from -6 to 6
- out_weight: bfloat16 [1024, 2048], replicated, may hold values from -0.1875 to 0.1875
- gain_mix: float32 [2048], replicated, may hold values from 0.1 to 1.9
- gain_pre: float32 [2048], replicated, may hold values from 0.1 to 1.9
- gain_post: float32 [2048], replicated, may hold values from 0.1 to 1.9
- route_ids: int32 [16384, 2], P(('sp', 'tp')), may hold values from 0 to 127, all different within a row; in each aligned block of 128 rows (0 to 127, 128 to 255, ...) at most 3 rows name the same one
- route_weight: float32 [16384, 2], P(('sp', 'tp')), may hold values from 0.2 to 1
- w_gate: bfloat16 [128, 2048, 512], P(('sp', 'tp')), may hold values from -0.125 to 0.125
- w_up: bfloat16 [128, 2048, 512], P(('sp', 'tp')), may hold values from -0.125 to 0.125
- w_down: bfloat16 [128, 512, 2048], P(('sp', 'tp')), may hold values from -0.25 to 0.25
Outputs:
- layer_out: bfloat16 [16384, 2048], P(('sp', 'tp'))
The draws below stay inside these ranges and needn't reach their ends.
Inputs may be any that keep to these rules, and one draw needn't show every extreme that they name: `route_ids`: each row names 2 different experts; in the rows of one device no expert is named more than 3 times, a bound that some block reaches. `cum_gate`: along the positions each head's values never rise.
All inputs are finite; a program needn't handle non-finite values.
Results may differ from the reference program's by a relative error of at most 0.018.
Values may be sent and summed in bfloat16 or wider, within the bound.
No kernel may reach another device: no remote copies, remote signals or barrier semaphores. Data moves between devices by JAX's collectives and lax.ppermute only.
A program may use at most 64 MiB of HBM per device.

```python
import math
import jax
import jax.numpy as jnp
import numpy as np
from jax import lax

D = 2048
ATTENTION_HEADS = 16
HEAD_DIM = 64
FF = 512
TOP = 2
TOK_DEV = 1024
TOKEN_COUNT = 16384
ROWS = 128
EXPERTS = 128
CAP = 3
N_SP = 16
N_TP = 8


def draw_queries(key, part):
    sample = jax.random.normal(jax.random.fold_in(key, 1), (TOKEN_COUNT, ATTENTION_HEADS * HEAD_DIM), jnp.float32)
    return jnp.clip(sample, -4.0, 4.0).astype(jnp.bfloat16)


def draw_key_rows(key, part):
    sample = jax.random.normal(jax.random.fold_in(key, 2), (TOKEN_COUNT, ATTENTION_HEADS * HEAD_DIM), jnp.float32)
    return jnp.clip(sample, -4.0, 4.0).astype(jnp.bfloat16)


def draw_cum_gate(key, part):
    key_o, key_s, key_f, key_r, key_b, random_key_position, random_key_log = jax.random.split(jax.random.fold_in(key, 5), 7)
    shuffle = jax.random.permutation(key_o, ATTENTION_HEADS)
    slow_head = shuffle < ATTENTION_HEADS // 2
    slow_total = jax.random.uniform(key_s, (ATTENTION_HEADS,), jnp.float32, 0.4, 1.0)
    fast_rate = jnp.exp(jax.random.uniform(key_f, (ATTENTION_HEADS,), jnp.float32, -4.6, -3.4))
    step_rate = jnp.where(slow_head, slow_total / TOKEN_COUNT, fast_rate)
    blocks = TOKEN_COUNT // TOK_DEV
    roughness = jnp.exp(jax.random.uniform(key_r, (ATTENTION_HEADS, blocks, TOK_DEV), jnp.float32, -0.7, 0.7))
    block_factor = jnp.exp(jax.random.uniform(key_b, (ATTENTION_HEADS, blocks, 1), jnp.float32, -0.7, 0.7))
    logarithm_steps = step_rate[:, None] * (roughness * block_factor).reshape(ATTENTION_HEADS, TOKEN_COUNT)
    spike_position = jax.random.randint(random_key_position, (ATTENTION_HEADS, 2), 0, TOKEN_COUNT)
    spike_decay = -jnp.log(1.0 - jax.random.uniform(random_key_log, (ATTENTION_HEADS, 2), jnp.float32, 0.2, 0.45))
    index_of_head = jnp.broadcast_to(lax.iota(jnp.int32, ATTENTION_HEADS)[:, None], (ATTENTION_HEADS, 2))
    logarithm_steps = logarithm_steps.at[index_of_head, spike_position].add(spike_decay)
    return -jnp.cumsum(logarithm_steps, axis=1)


def steps_of(own_key, extent, cuts, least, high):
    def one(position, parts):
        draws = jax.random.uniform(jax.random.fold_in(jax.random.fold_in(own_key, 6), position), (parts,), jnp.float32, least / len(cuts), high / len(cuts))
        return jnp.repeat(jnp.exp(draws), extent[position] // parts).reshape((-1,) + (1,) * (len(extent) - position - 1))

    level = one(*cuts[0])
    for cut in cuts[1:]:
        level = level * one(*cut)
    return level


def shared_out(own_key, own, number, rows, number_of, top, bound, skew):
    ranking = jax.random.permutation(own_key, number_of)
    heavy_load, ordinary = shares(number_of, rows * top, bound, skew, True), shares(number_of, rows * top, bound, skew, False)
    places = jnp.arange(number_of)

    def named(lengths, offset_by):
        used = int((lengths > 0).sum())
        fixed = max(1, used // 4)
        passed = fixed + (places - fixed + offset_by * (used - fixed)) % max(1, number_of - fixed)
        return jnp.zeros((number_of,), jnp.int32).at[ranking[jnp.where(places < fixed, places, passed)]].set(jnp.asarray(lengths, jnp.int32))

    lengths = jnp.where(number % 4 == 0, named(heavy_load, number // 4), named(ordinary, number - number // 4 - 1))
    mixed = jax.random.permutation(jax.random.fold_in(own, 3), number_of)
    source_of, taker = mixed[0:number_of // 2 * 2:2], mixed[1:number_of // 2 * 2:2]
    slack = jnp.minimum(lengths[source_of] - 1, bound - lengths[taker]) // 2
    slack = jnp.where((source_of == ranking[0]) | (taker == ranking[0]) | (lengths[taker] == 0), 0, jnp.maximum(slack, 0))
    passed = jax.random.randint(jax.random.fold_in(own, 4), (number_of // 2,), 0, 1 << 20) % (slack + 1)
    lengths = lengths.at[source_of].add(-passed).at[taker].add(passed)
    labels = jnp.searchsorted(jnp.cumsum(lengths), jnp.arange(rows * top), side="right").astype(jnp.int32)
    grid = labels.reshape(top, rows).T
    grid = grid[jax.random.permutation(jax.random.fold_in(own, 1), rows)]
    offset_by = jax.random.randint(jax.random.fold_in(own, 2), (rows, 1), 0, top)
    return jnp.take_along_axis(grid, (jnp.arange(top)[None, :] + offset_by) % top, axis=1)


def shares(count, total, reach, skew, full):
    portions = [(1 << 20) // math.isqrt(rank ** skew) + 1 for rank in range(1, count + 1)]
    largest = reach if full else min(reach, max(-(-total // count), total * portions[0] // sum(portions)))
    least = 1 if total - largest >= count - 1 else 0
    holding, spare = [largest] + [least] * (count - 1), total - largest - least * (count - 1)
    while spare > 0:
        free = [i for i in range(1, count) if holding[i] < largest] or [i for i in range(1, count) if holding[i] < reach]
        pool, remaining = sum([portions[i] for i in free]), spare
        for i in free:
            more = min(reach - holding[i], max(1, remaining * portions[i] // pool), spare)
            holding[i] = holding[i] + more
            spare = spare - more
    return np.array(holding)


def scatter_about(own_key, dims, deviation, reach, shards=(), kind=jnp.bfloat16):
    values = jax.random.normal(own_key, dims, jnp.float32) * deviation
    if len(shards) > 0:
        values = steps_of(own_key, dims, shards, -0.22, 0.18) * values
    return jnp.clip(values, min=-reach, max=reach).astype(kind)


def setup_inputs(seed: int = 0) -> dict:
    keys = jax.random.split(jax.random.key(seed), 15)
    queries = draw_queries(jax.random.fold_in(keys[14], 71), 0)
    key_rows = draw_key_rows(jax.random.fold_in(keys[14], 71), 0)
    value_rows = scatter_about(keys[2], (TOKEN_COUNT, ATTENTION_HEADS * HEAD_DIM), 1.0, 6.0, ((0, 16), (1, 8)))
    cum_gate = draw_cum_gate(jax.random.fold_in(keys[14], 71), 0)
    residual = scatter_about(keys[4], (TOKEN_COUNT, D), 1.0, 6.0, ((0, 128),))
    out_weight = scatter_about(keys[5], (ATTENTION_HEADS * HEAD_DIM, D), (ATTENTION_HEADS * HEAD_DIM) ** -0.5, 0.1875)
    gain_mix = jnp.clip(1.0 + 0.18 * jax.random.normal(keys[6], (D,), jnp.float32), 0.1, 1.9)
    gain_pre = jnp.clip(1.0 + 0.18 * jax.random.normal(keys[7], (D,), jnp.float32), 0.1, 1.9)
    gain_post = jnp.clip(1.0 + 0.18 * jax.random.normal(keys[8], (D,), jnp.float32), 0.1, 1.9)
    route_ids_keys = jax.random.split(jax.random.fold_in(keys[9], 1), TOKEN_COUNT // ROWS)
    route_ids_turns = jax.random.permutation(jax.random.fold_in(keys[9], 3), TOKEN_COUNT // ROWS)
    route_ids = jax.vmap(lambda own, number: shared_out(jax.random.fold_in(keys[9], 2), own, number, ROWS, EXPERTS, TOP, CAP, 1))(route_ids_keys, route_ids_turns).reshape((TOKEN_COUNT, TOP))
    route_weight = jnp.clip(jnp.exp(math.log(1.0) - 1.609438 * jax.random.uniform(keys[10], (TOKEN_COUNT, TOP), jnp.float32) ** steps_of(keys[10], (TOKEN_COUNT, TOP), ((0, 128),), -0.2, 0.2)), 0.2, 1.0)
    w_gate = scatter_about(keys[11], (EXPERTS, D, FF), D ** -0.5, 0.125, ((0, 128),))
    w_up = scatter_about(keys[12], (EXPERTS, D, FF), D ** -0.5, 0.125, ((0, 128),))
    w_down = scatter_about(keys[13], (EXPERTS, FF, D), FF ** -0.5, 0.25, ((0, 128),))
    return {"queries": queries, "key_rows": key_rows, "value_rows": value_rows, "cum_gate": cum_gate, "residual": residual, "out_weight": out_weight, "gain_mix": gain_mix, "gain_pre": gain_pre, "gain_post": gain_post, "route_ids": route_ids, "route_weight": route_weight, "w_gate": w_gate, "w_up": w_up, "w_down": w_down}


NORM_EPS = 1e-06
MASKED = -1e+30

def rms_scale(rows, gain):
    mean_sq = lax.optimization_barrier(jnp.mean(rows * rows, axis=-1, keepdims=True))
    return rows * lax.rsqrt(mean_sq + NORM_EPS) * gain

def attend(running, queries, gate_q, q_start, key_part, value_part, gate_k, k_start):
    row_peak, row_total, weighted = running
    scores = jnp.einsum('qhd,khd->hqk', queries.astype(jnp.float32), key_part.astype(jnp.float32)) * HEAD_DIM ** (-0.5)
    scores = scores + gate_q[:, :, None] - gate_k[:, None, :]
    query_pos = q_start + lax.iota(jnp.int32, queries.shape[0])
    key_pos = k_start + lax.iota(jnp.int32, key_part.shape[0])
    allowed = (key_pos[None, :] <= query_pos[:, None])[None]
    scores = jnp.where(allowed, scores, MASKED)
    new_peak = jnp.maximum(row_peak, lax.optimization_barrier(jnp.max(scores, axis=-1)))
    unnorm = jnp.where(allowed, jnp.exp(scores - new_peak[..., None]), 0.0)
    rescale = jnp.exp(row_peak - new_peak)
    row_total = row_total * rescale + lax.optimization_barrier(jnp.sum(unnorm, axis=-1))
    probs = lax.optimization_barrier(unnorm.astype(jnp.bfloat16)).astype(jnp.float32)
    weighted = weighted * rescale.T[:, :, None] + jnp.einsum('hqk,khd->qhd', probs, value_part.astype(jnp.float32))
    return (new_peak, row_total, weighted)

def attention(queries, key_rows, value_rows, cum_gate):
    query_heads = queries.reshape(TOKEN_COUNT, ATTENTION_HEADS, HEAD_DIM)
    key_heads = key_rows.reshape(TOKEN_COUNT, ATTENTION_HEADS, HEAD_DIM)
    value_heads = value_rows.reshape(TOKEN_COUNT, ATTENTION_HEADS, HEAD_DIM)

    def one_block(block_index):
        q_start = block_index * TOK_DEV
        query_block = lax.dynamic_slice_in_dim(query_heads, q_start, TOK_DEV, 0)
        gate_q = lax.dynamic_slice_in_dim(cum_gate, q_start, TOK_DEV, 1)
        initial = (jnp.full((ATTENTION_HEADS, TOK_DEV), MASKED, jnp.float32), jnp.zeros((ATTENTION_HEADS, TOK_DEV), jnp.float32), jnp.zeros((TOK_DEV, ATTENTION_HEADS, HEAD_DIM), jnp.float32))

        def key_block(other, running):
            k_start = (other * TOK_DEV).astype(jnp.int32)
            return attend(running, query_block, gate_q, q_start, lax.dynamic_slice_in_dim(key_heads, k_start, TOK_DEV, 0), lax.dynamic_slice_in_dim(value_heads, k_start, TOK_DEV, 0), lax.dynamic_slice_in_dim(cum_gate, k_start, TOK_DEV, 1), k_start)
        row_peak, row_total, weighted = lax.fori_loop(jnp.int32(0), block_index + 1, key_block, initial)
        return (weighted / row_total.T[:, :, None]).astype(jnp.bfloat16)
    blocks = lax.map(one_block, jnp.arange(N_SP, dtype=jnp.int32))
    return blocks.reshape(TOKEN_COUNT, ATTENTION_HEADS * HEAD_DIM)

def route_experts(normed, route_ids, route_weight, w_gate, w_up, w_down):
    sources = N_SP * N_TP
    flat_ids = route_ids.reshape(sources, ROWS * TOP)
    onehot = (flat_ids[:, :, None] == jnp.arange(EXPERTS, dtype=jnp.int32)[None, None, :]).astype(jnp.int32)
    slot_rank = (lax.optimization_barrier(jnp.sum(jnp.cumsum(onehot, axis=1) * onehot, axis=2)) - 1).astype(jnp.int32)
    slot_index = flat_ids * (sources * CAP) + jnp.arange(sources, dtype=jnp.int32)[:, None] * CAP + slot_rank
    slot_index = slot_index.reshape(-1).astype(jnp.int32)
    token_index = jnp.arange(TOKEN_COUNT * TOP, dtype=jnp.int32) // TOP
    slot_count = EXPERTS * sources * CAP
    source_row = jnp.zeros((slot_count,), jnp.int32).at[slot_index].set(token_index)
    slot_weight = jnp.zeros((slot_count,), jnp.float32).at[slot_index].set(route_weight.reshape(-1))

    def one_expert(summed, expert):
        offset = (expert * sources * CAP).astype(jnp.int32)
        picked_rows = lax.dynamic_slice_in_dim(source_row, offset, sources * CAP)
        weights = lax.dynamic_slice_in_dim(slot_weight, offset, sources * CAP)
        routed = normed[picked_rows]
        gate_act = jnp.dot(routed, w_gate[expert], preferred_element_type=jnp.float32)
        up_act = jnp.dot(routed, w_up[expert], preferred_element_type=jnp.float32)
        hidden = (jax.nn.silu(gate_act) * up_act).astype(jnp.bfloat16)
        result = jnp.dot(hidden, w_down[expert], preferred_element_type=jnp.float32).astype(jnp.bfloat16)
        summed = summed.at[picked_rows].add(weights[:, None] * result.astype(jnp.float32))
        return (summed, None)
    summed, _ = lax.scan(one_expert, jnp.zeros((TOKEN_COUNT, D), jnp.float32), jnp.arange(EXPERTS, dtype=jnp.int32))
    return summed

def reference(queries, key_rows, value_rows, cum_gate, residual, out_weight, gain_mix, gain_pre, gain_post, route_ids, route_weight, w_gate, w_up, w_down):
    attended = attention(queries, key_rows, value_rows, cum_gate)
    projected = jnp.dot(attended, out_weight, preferred_element_type=jnp.float32)
    stream = (residual.astype(jnp.float32) + rms_scale(projected, gain_mix)).astype(jnp.bfloat16)
    stream_wide = lax.optimization_barrier(stream).astype(jnp.float32)
    normed = rms_scale(stream_wide, gain_pre).astype(jnp.bfloat16)
    combined = route_experts(normed, route_ids, route_weight, w_gate, w_up, w_down)
    return (stream_wide + rms_scale(combined, gain_post)).astype(jnp.bfloat16)
```

```python
import functools

import jax
import jax.numpy as jnp
from jax import lax
from jax.experimental import pallas as pl
from jax.experimental.pallas import tpu as pltpu
from jax.sharding import PartitionSpec as P

HEAD_DIM = 64
NORM_EPS = 1e-06
MASKED = -1e30
BF = jnp.bfloat16
F32 = jnp.float32
ALL = ("sp", "tp")
BLK = 1024
TILE = 128
QG = 512


def member(k, z):
    return 4 * z + (k if z % 2 == 0 else 3 - k)


def group_of(sp):
    z, x = divmod(sp, 4)
    return x if z % 2 == 0 else 3 - x


def exchange_pairs(m1, m2):
    pairs = []
    for sp in range(16):
        z = sp // 4
        for tp in range(8):
            y, s = divmod(tp, 2)
            to_z = 2 * s + (m1 ^ (z & 1))
            to_c = m2 ^ (z >> 1)
            pairs.append((sp * 8 + tp, member(group_of(sp), to_z) * 8 + 2 * y + to_c))
    return pairs


def ring_pairs(step):
    return [(sp, 4 * (sp // 4) + (sp % 4 + step) % 4) for sp in range(16)]


def out_groups():
    return [
        [member(k, z) * 8 + 2 * y + c for z in range(4) for y in range(4)]
        for k in range(4)
        for c in range(2)
    ]


CORE_PAIRS = [(i, i ^ 1) for i in range(8)]


def pack_kernel(meta, q_ref, k_ref, v_ref, *outs):
    z = meta[0]
    row = lax.broadcasted_iota(jnp.int32, (128, 128), 0)
    col = lax.broadcasted_iota(jnp.int32, (128, 128), 1)
    for m1 in range(2):
        f1 = m1 ^ (z & 1)
        low = jnp.where((col < 64) & (row == col + 64 * f1), 1.0, 0.0)
        high = jnp.where((col >= 64) & (row == col - 64 + 64 * f1), 1.0, 0.0)
        sel_lo, sel_hi = low.astype(BF), high.astype(BF)
        q_lo, q_hi = (low * 0.125).astype(BF), (high * 0.125).astype(BF)

        def dot(a, b):
            return jnp.dot(a, b, preferred_element_type=F32)

        for m2 in range(2):
            f2 = m2 ^ (z >> 1)
            out = outs[2 * m1 + m2]
            for i in range(4):
                src = pl.ds(pl.multiple_of((2 * i + f2) * TILE, TILE), TILE)
                kv = dot(k_ref[src, :], sel_lo) + dot(v_ref[src, :], sel_hi)
                out[i * TILE : (i + 1) * TILE, :] = kv.astype(BF)
            for i in range(2):
                src_a = pl.ds(pl.multiple_of((2 * i + f2) * TILE, TILE), TILE)
                src_b = pl.ds(pl.multiple_of((2 * i + 4 + f2) * TILE, TILE), TILE)
                qq = dot(q_ref[src_a, :], q_lo) + dot(q_ref[src_b, :], q_hi)
                out[QG + i * TILE : QG + (i + 1) * TILE, :] = qq.astype(BF)


def pack(meta, q, k, v):
    return pl.pallas_call(
        pack_kernel,
        in_specs=[pl.BlockSpec(memory_space=pltpu.SMEM)] + [pl.BlockSpec(memory_space=pltpu.VMEM)] * 3,
        out_shape=[jax.ShapeDtypeStruct((768, 128), BF)] * 4,
        out_specs=[pl.BlockSpec(memory_space=pltpu.VMEM)] * 4,
        name="pack",
    )(meta, q, k, v)


def attend_kernel(n_pairs, first, last, meta, *refs):
    refs = list(refs)
    gate_own, gate_peer = refs.pop(0), refs.pop(0)
    qs = [refs.pop(0) for _ in range(4)]
    kv_in = [refs.pop(0) for _ in range(2 * n_pairs)]
    if not first:
        m_in, acc_in = refs.pop(0), refs.pop(0)
    if last:
        out_ref = refs.pop(0)
        m_ref, acc_ref = None, None
    else:
        m_ref, acc_ref = refs.pop(0), refs.pop(0)
    kv, q_pad, gate, sems = refs.pop(0), refs.pop(0), refs.pop(0), refs.pop(0)
    if last:
        m_ref, acc_ref = refs.pop(0), refs.pop(0)
    z, x, core = meta[0], meta[1], meta[2]

    copies = []
    for i, src in enumerate(kv_in):
        copies.append(pltpu.make_async_copy(src, kv.at[pl.ds(i * 2048, 2048)], sems.at[i]))
        copies[-1].start()

    mine = lax.shift_right_logical(z, 1) == core
    row0 = pl.multiple_of((z & 1) * 128, 128)
    gate[...] = jnp.where(mine, gate_own[pl.ds(row0, 128), :], gate_peer[pl.ds(row0, 128), :])

    lane = lax.broadcasted_iota(jnp.int32, (256, 128), 1)
    for g in range(4):
        packed = qs[g][...].astype(F32)
        q_pad[g, 0:256, :] = jnp.where(lane < 64, packed, 0.0).astype(BF)
        q_pad[g, 256:512, :] = jnp.where(lane < 64, pltpu.roll(packed, 64, 1), 0.0).astype(BF)
    if first:
        m_ref[...] = jnp.full(m_ref.shape, MASKED, F32)
        acc_ref[...] = jnp.zeros(acc_ref.shape, F32)
    else:
        m_ref[...] = m_in[...]
        acc_ref[...] = acc_in[...]

    def block_of(m1, m2, parity, x_of):
        zb = (m1 ^ (z & 1)) + 2 * (m2 ^ parity)
        xb = jnp.where(m1 == 1, 3 - x_of, x_of)
        return zb, 4 * zb + xb

    def step(g, base, m1, m2, b_q, b_k, masked):
        start_a = pl.multiple_of(base + (2 * m1 + m2) * QG, QG)
        start_b = pl.multiple_of(base + 2048 + (2 * m1 + (1 - m2)) * QG, QG)
        kv_a, kv_b = kv[pl.ds(start_a, QG), :], kv[pl.ds(start_b, QG), :]
        ones = lax.broadcasted_iota(jnp.int32, (QG, 128), 1) < 64
        v_a = jnp.where(ones, jnp.ones_like(kv_a), kv_a)
        v_b = jnp.where(ones, jnp.ones_like(kv_b), kv_b)
        ref_gate = gate[pl.ds(b_q * 8, 1), 0:1]

        def gates(parity):
            parts = [gate[pl.ds(b_k * 8 + 2 * i + parity, 1), :] for i in range(4)]
            return jnp.concatenate(parts, axis=1) - ref_gate

        g_a, g_b = gates(core), gates(1 - core)
        for sub in range(2):
            rows = slice(sub * 256, sub * 256 + 256)
            q = q_pad[g, rows, :]
            nt = (((1,), (1,)), ((), ()))
            s_a = lax.dot_general(q, kv_a, nt, preferred_element_type=F32) - g_a
            s_b = lax.dot_general(q, kv_b, nt, preferred_element_type=F32) - g_b
            if masked:
                r = lax.broadcasted_iota(jnp.int32, (256, QG), 0) + sub * 256
                cc = lax.broadcasted_iota(jnp.int32, (256, QG), 1)
                qpos = lax.shift_right_logical(r, 7) * 256 + (r & 127) + core * 128
                kpos = lax.shift_right_logical(cc, 7) * 256 + (cc & 127)
                s_a = jnp.where(kpos + core * 128 <= qpos, s_a, MASKED)
                s_b = jnp.where(kpos + (1 - core) * 128 <= qpos, s_b, MASKED)
            m_old = m_ref[g, rows, :]
            top = jnp.maximum(jnp.max(s_a, axis=1, keepdims=True), jnp.max(s_b, axis=1, keepdims=True))
            m_new = jnp.maximum(m_old, top)
            m_col = m_new[:, 0:1]
            p_a = jnp.exp(s_a - m_col).astype(BF)
            p_b = jnp.exp(s_b - m_col).astype(BF)
            pv = jnp.dot(p_a, v_a, preferred_element_type=F32) + jnp.dot(p_b, v_b, preferred_element_type=F32)
            acc_ref[g, rows, :] = acc_ref[g, rows, :] * jnp.exp(m_old - m_new) + pv
            m_ref[g, rows, :] = m_new

    for i in range(n_pairs):
        copies[2 * i].wait()
        copies[2 * i + 1].wait()
        x_of = meta[3 + i]

        def body(t, _, i=i, x_of=x_of):
            g, slot = t // 4, t % 4
            _, b_q = block_of(g // 2, g % 2, core, x)
            _, b_k = block_of(slot // 2, slot % 2, core, x_of)

            @pl.when(b_k < b_q)
            def _():
                step(g, i * 4096, slot // 2, slot % 2, b_q, b_k, False)

            if first and i == 0:

                @pl.when(b_k == b_q)
                def _():
                    step(g, i * 4096, slot // 2, slot % 2, b_q, b_k, True)

            return 0

        lax.fori_loop(0, 16, body, 0)

    if last:

        def finish(g, _):
            zq, _b = block_of(g // 2, g % 2, core, x)
            lane64 = lax.broadcasted_iota(jnp.int32, (64, 128), 1) < 64
            for i in range(4):
                a = acc_ref[g, i * TILE : (i + 1) * TILE, :]
                o = a / a[:, 0:1]
                packed = jnp.where(lane64, pltpu.roll(o[0:64], 64, 1), o[64:128])
                out_ref[zq * 4 + i, :, :] = packed.astype(BF)
            return 0

        lax.fori_loop(0, 4, finish, 0)


def attend(meta, gates, qs, kvs, state=None, last=True):
    n_pairs = len(kvs) // 2
    first = state is None
    vmem = pl.BlockSpec(memory_space=pltpu.VMEM)
    hbm = pl.BlockSpec(memory_space=pl.ANY)
    args = [meta, *gates, *qs, *kvs]
    specs = [pl.BlockSpec(memory_space=pltpu.SMEM)] + [vmem] * 6 + [hbm] * len(kvs)
    if not first:
        args += list(state)
        specs += [vmem, vmem]
    pair = (4, QG, 128)
    if last:
        out_shape = jax.ShapeDtypeStruct((16, 64, 128), BF)
        out_specs = vmem
    else:
        out_shape = [jax.ShapeDtypeStruct(pair, F32)] * 2
        out_specs = [vmem, vmem]
    scratch = [
        pltpu.VMEM((4096 * n_pairs, 128), BF),
        pltpu.VMEM((4, QG, 128), BF),
        pltpu.VMEM((128, 128), F32),
        pltpu.SemaphoreType.DMA((2 * n_pairs,)),
    ]
    if last:
        scratch += [pltpu.VMEM(pair, F32), pltpu.VMEM(pair, F32)]
    return pl.pallas_call(
        functools.partial(attend_kernel, n_pairs, first, last),
        in_specs=specs,
        out_shape=out_shape,
        out_specs=out_specs,
        scratch_shapes=scratch,
        name="attend",
    )(*args)


def rms_scale(rows, gain):
    mean_sq = jnp.mean(rows * rows, axis=-1, keepdims=True)
    return rows * lax.rsqrt(mean_sq + NORM_EPS) * gain


def attention(queries, key_rows, value_rows, cum_gate):
    sp, tp = lax.axis_index("sp"), lax.axis_index("tp")
    z, x, core = sp // 4, sp % 4, tp % 2
    left, right, far = (x + 3) % 4, (x + 1) % 4, (x + 2) % 4
    gate_own = cum_gate.reshape(256, 128)
    gate_peer = lax.ppermute(gate_own, "tp", CORE_PAIRS)
    meta = jnp.stack([z, x, core, x, left, right, far]).astype(jnp.int32)
    msgs = pack(meta, queries, key_rows, value_rows)
    recv = [
        lax.ppermute(msgs[2 * m1 + m2], ALL, exchange_pairs(m1, m2))
        for m1 in range(2)
        for m2 in range(2)
    ]
    qs = [r[QG:] for r in recv]
    own = jnp.concatenate([r[:QG] for r in recv], axis=0)

    def swap(a):
        return lax.ppermute(a, "tp", CORE_PAIRS)

    from_left = lax.ppermute(own, "sp", ring_pairs(1))
    from_right = lax.ppermute(own, "sp", ring_pairs(-1))
    peer = swap(own)
    far_a = lax.ppermute(from_left[:1024], "sp", ring_pairs(1))
    far_b = lax.ppermute(from_right[1024:], "sp", ring_pairs(-1))
    left_peer, right_peer = swap(from_left), swap(from_right)
    far_own = jnp.concatenate([far_a, far_b], axis=0)
    far_peer = swap(far_own)
    out = attend(
        meta,
        (gate_own, gate_peer),
        qs,
        [own, peer, from_left, left_peer, from_right, right_peer, far_own, far_peer],
    )
    got = lax.all_to_all(out, ALL, split_axis=0, concat_axis=0, tiled=True, axis_index_groups=out_groups())
    got = got.reshape(4, 4, 64, 2, 64)
    return jnp.transpose(got, (3, 2, 1, 0, 4)).reshape(TILE, 1024)


def local(
    queries,
    key_rows,
    value_rows,
    cum_gate,
    residual,
    out_weight,
    gain_mix,
    gain_pre,
    gain_post,
    route_ids,
    route_weight,
    w_gate,
    w_up,
    w_down,
):
    head_rows = attention(queries, key_rows, value_rows, cum_gate)
    projected = jnp.dot(head_rows, out_weight, preferred_element_type=jnp.float32)
    stream = (residual.astype(jnp.float32) + rms_scale(projected, gain_mix)).astype(jnp.bfloat16)
    stream_wide = lax.optimization_barrier(stream).astype(jnp.float32)
    normed = rms_scale(stream_wide, gain_pre).astype(jnp.bfloat16)
    rows_dev, top_count = route_ids.shape
    model_width = normed.shape[1]
    experts_all = lax.axis_size("sp") * lax.axis_size("tp")
    capacity = max(2, (4 * rows_dev * top_count + 3 * experts_all - 1) // (3 * experts_all))
    flat_ids = route_ids.reshape(-1)
    onehot = (flat_ids[:, None] == lax.iota(jnp.int32, experts_all)[None, :]).astype(jnp.int32)
    slot_rank = jnp.sum(jnp.cumsum(onehot, axis=0) * onehot, axis=1) - 1
    slot_index = flat_ids * capacity + slot_rank
    spread = jnp.repeat(normed, top_count, axis=0)
    outgoing = (
        jnp.zeros((experts_all * capacity, model_width), jnp.bfloat16).at[slot_index].set(spread)
    )
    outgoing = outgoing.reshape(experts_all, capacity, model_width)
    arrived = lax.all_to_all(outgoing, ("sp", "tp"), split_axis=0, concat_axis=0, tiled=True)
    sources, slots, width_here = arrived.shape
    flat_rows = arrived.reshape(sources * slots, width_here)
    gate_act = jnp.dot(flat_rows, w_gate[0], preferred_element_type=jnp.float32)
    up_act = jnp.dot(flat_rows, w_up[0], preferred_element_type=jnp.float32)
    hidden = (jax.nn.silu(gate_act) * up_act).astype(jnp.bfloat16)
    expert_out = jnp.dot(hidden, w_down[0], preferred_element_type=jnp.float32).astype(jnp.bfloat16)
    returned = lax.all_to_all(
        expert_out.reshape(sources, slots, width_here),
        ("sp", "tp"),
        split_axis=0,
        concat_axis=0,
        tiled=True,
    )
    picked = returned.reshape(experts_all * capacity, model_width)[slot_index]
    picked = picked.reshape(rows_dev, top_count, model_width).astype(jnp.float32)
    combined = jnp.sum(picked * route_weight[:, :, None], axis=1)
    return (stream_wide + rms_scale(combined, gain_post)).astype(jnp.bfloat16)


def solution(mesh):
    return jax.shard_map(
        local,
        mesh=mesh,
        in_specs=(
            P("sp", "tp"),
            P("sp", "tp"),
            P("sp", "tp"),
            P("tp", None),
            P(("sp", "tp"), None),
            P(),
            P(),
            P(),
            P(),
            P(("sp", "tp"), None),
            P(("sp", "tp"), None),
            P(("sp", "tp"), None, None),
            P(("sp", "tp"), None, None),
            P(("sp", "tp"), None, None),
        ),
        out_specs=P(("sp", "tp"), None),
        check_vma=False,
    )
```

```python
import functools

import jax
import jax.numpy as jnp
from jax import lax
from jax.experimental import pallas as pl
from jax.experimental.pallas import tpu as pltpu
from jax.sharding import PartitionSpec as P

HEAD_DIM = 64
NORM_EPS = 1e-06
MASKED = -1e30
BF = jnp.bfloat16
F32 = jnp.float32
ALL = ("sp", "tp")
BLK = 1024
TILE = 128
QG = 512


def member(k, z):
    return 4 * z + (k if z % 2 == 0 else 3 - k)


def group_of(sp):
    z, x = divmod(sp, 4)
    return x if z % 2 == 0 else 3 - x


def exchange_pairs(m1, m2):
    pairs = []
    for sp in range(16):
        z = sp // 4
        for tp in range(8):
            y, s = divmod(tp, 2)
            to_z = 2 * s + (m1 ^ (z & 1))
            to_c = m2 ^ (z >> 1)
            pairs.append((sp * 8 + tp, member(group_of(sp), to_z) * 8 + 2 * y + to_c))
    return pairs


def ring_pairs(step):
    return [(sp, 4 * (sp // 4) + (sp % 4 + step) % 4) for sp in range(16)]


def out_groups():
    return [
        [member(k, z) * 8 + 2 * y + c for z in range(4) for y in range(4)]
        for k in range(4)
        for c in range(2)
    ]


CORE_PAIRS = [(i, i ^ 1) for i in range(8)]


def pack_kernel(meta, q_ref, k_ref, v_ref, *outs):
    z = meta[0]
    row = lax.broadcasted_iota(jnp.int32, (128, 128), 0)
    col = lax.broadcasted_iota(jnp.int32, (128, 128), 1)
    for m1 in range(2):
        f1 = m1 ^ (z & 1)
        low = jnp.where((col < 64) & (row == col + 64 * f1), 1.0, 0.0)
        high = jnp.where((col >= 64) & (row == col - 64 + 64 * f1), 1.0, 0.0)
        sel_lo, sel_hi = low.astype(BF), high.astype(BF)
        q_lo, q_hi = (low * 0.125).astype(BF), (high * 0.125).astype(BF)

        def dot(a, b):
            return jnp.dot(a, b, preferred_element_type=F32)

        for m2 in range(2):
            f2 = m2 ^ (z >> 1)
            out = outs[2 * m1 + m2]
            for i in range(4):
                src = pl.ds(pl.multiple_of((2 * i + f2) * TILE, TILE), TILE)
                kv = dot(k_ref[src, :], sel_lo) + dot(v_ref[src, :], sel_hi)
                out[i * TILE : (i + 1) * TILE, :] = kv.astype(BF)
            for i in range(2):
                src_a = pl.ds(pl.multiple_of((2 * i + f2) * TILE, TILE), TILE)
                src_b = pl.ds(pl.multiple_of((2 * i + 4 + f2) * TILE, TILE), TILE)
                qq = dot(q_ref[src_a, :], q_lo) + dot(q_ref[src_b, :], q_hi)
                out[QG + i * TILE : QG + (i + 1) * TILE, :] = qq.astype(BF)


def pack(meta, q, k, v):
    return pl.pallas_call(
        pack_kernel,
        in_specs=[pl.BlockSpec(memory_space=pltpu.SMEM)] + [pl.BlockSpec(memory_space=pltpu.VMEM)] * 3,
        out_shape=[jax.ShapeDtypeStruct((768, 128), BF)] * 4,
        out_specs=[pl.BlockSpec(memory_space=pltpu.VMEM)] * 4,
        name="pack",
    )(meta, q, k, v)


def attend_kernel(n_pairs, first, last, meta, *refs):
    refs = list(refs)
    gate_own, gate_peer = refs.pop(0), refs.pop(0)
    qs = [refs.pop(0) for _ in range(4)]
    kv_in = [refs.pop(0) for _ in range(2 * n_pairs)]
    if not first:
        m_in, acc_in = refs.pop(0), refs.pop(0)
    if last:
        out_ref = refs.pop(0)
        m_ref, acc_ref = None, None
    else:
        m_ref, acc_ref = refs.pop(0), refs.pop(0)
    kv, q_pad, gate, sems = refs.pop(0), refs.pop(0), refs.pop(0), refs.pop(0)
    if last:
        m_ref, acc_ref = refs.pop(0), refs.pop(0)
    z, x, core = meta[0], meta[1], meta[2]

    copies = []
    for i, src in enumerate(kv_in):
        copies.append(pltpu.make_async_copy(src, kv.at[pl.ds(i * 2048, 2048)], sems.at[i]))
        copies[-1].start()

    mine = lax.shift_right_logical(z, 1) == core
    row0 = pl.multiple_of((z & 1) * 128, 128)
    gate[...] = jnp.where(mine, gate_own[pl.ds(row0, 128), :], gate_peer[pl.ds(row0, 128), :])

    lane = lax.broadcasted_iota(jnp.int32, (256, 128), 1)
    for g in range(4):
        packed = qs[g][...].astype(F32)
        q_pad[g, 0:256, :] = jnp.where(lane < 64, packed, 0.0).astype(BF)
        q_pad[g, 256:512, :] = jnp.where(lane < 64, pltpu.roll(packed, 64, 1), 0.0).astype(BF)
    if first:
        m_ref[...] = jnp.full(m_ref.shape, MASKED, F32)
        acc_ref[...] = jnp.zeros(acc_ref.shape, F32)
    else:
        m_ref[...] = m_in[...]
        acc_ref[...] = acc_in[...]

    def block_of(m1, m2, parity, x_of):
        zb = (m1 ^ (z & 1)) + 2 * (m2 ^ parity)
        xb = jnp.where(m1 == 1, 3 - x_of, x_of)
        return zb, 4 * zb + xb

    def step(g, base, m1, m2, b_q, b_k, masked):
        start_a = pl.multiple_of(base + (2 * m1 + m2) * QG, QG)
        start_b = pl.multiple_of(base + 2048 + (2 * m1 + (1 - m2)) * QG, QG)
        kv_a, kv_b = kv[pl.ds(start_a, QG), :], kv[pl.ds(start_b, QG), :]
        ones = lax.broadcasted_iota(jnp.int32, (QG, 128), 1) < 64
        v_a = jnp.where(ones, jnp.ones_like(kv_a), kv_a)
        v_b = jnp.where(ones, jnp.ones_like(kv_b), kv_b)
        ref_gate = gate[pl.ds(b_q * 8, 1), 0:1]

        def gates(parity):
            parts = [gate[pl.ds(b_k * 8 + 2 * i + parity, 1), :] for i in range(4)]
            return jnp.concatenate(parts, axis=1) - ref_gate

        g_a, g_b = gates(core), gates(1 - core)
        for sub in range(2):
            rows = slice(sub * 256, sub * 256 + 256)
            q = q_pad[g, rows, :]
            nt = (((1,), (1,)), ((), ()))
            s_a = lax.dot_general(q, kv_a, nt, preferred_element_type=F32) - g_a
            s_b = lax.dot_general(q, kv_b, nt, preferred_element_type=F32) - g_b
            if masked:
                r = lax.broadcasted_iota(jnp.int32, (256, QG), 0) + sub * 256
                cc = lax.broadcasted_iota(jnp.int32, (256, QG), 1)
                qpos = lax.shift_right_logical(r, 7) * 256 + (r & 127) + core * 128
                kpos = lax.shift_right_logical(cc, 7) * 256 + (cc & 127)
                s_a = jnp.where(kpos + core * 128 <= qpos, s_a, MASKED)
                s_b = jnp.where(kpos + (1 - core) * 128 <= qpos, s_b, MASKED)
            m_old = m_ref[g, rows, :]
            top = jnp.maximum(jnp.max(s_a, axis=1, keepdims=True), jnp.max(s_b, axis=1, keepdims=True))
            m_new = jnp.maximum(m_old, top)
            m_col = m_new[:, 0:1]
            p_a = jnp.exp(s_a - m_col).astype(BF)
            p_b = jnp.exp(s_b - m_col).astype(BF)
            pv = jnp.dot(p_a, v_a, preferred_element_type=F32) + jnp.dot(p_b, v_b, preferred_element_type=F32)
            acc_ref[g, rows, :] = acc_ref[g, rows, :] * jnp.exp(m_old - m_new) + pv
            m_ref[g, rows, :] = m_new

    for i in range(n_pairs):
        copies[2 * i].wait()
        copies[2 * i + 1].wait()
        x_of = meta[3 + i]

        def body(t, _, i=i, x_of=x_of):
            g, slot = t // 4, t % 4
            _, b_q = block_of(g // 2, g % 2, core, x)
            _, b_k = block_of(slot // 2, slot % 2, core, x_of)

            @pl.when(b_k < b_q)
            def _():
                step(g, i * 4096, slot // 2, slot % 2, b_q, b_k, False)

            if first and i == 0:

                @pl.when(b_k == b_q)
                def _():
                    step(g, i * 4096, slot // 2, slot % 2, b_q, b_k, True)

            return 0

        lax.fori_loop(0, 16, body, 0)

    if last:

        def finish(g, _):
            zq, _b = block_of(g // 2, g % 2, core, x)
            lane64 = lax.broadcasted_iota(jnp.int32, (64, 128), 1) < 64
            for i in range(4):
                a = acc_ref[g, i * TILE : (i + 1) * TILE, :]
                o = a / a[:, 0:1]
                packed = jnp.where(lane64, pltpu.roll(o[0:64], 64, 1), o[64:128])
                out_ref[zq * 4 + i, :, :] = packed.astype(BF)
            return 0

        lax.fori_loop(0, 4, finish, 0)


def attend(meta, gates, qs, kvs, state=None, last=True):
    n_pairs = len(kvs) // 2
    first = state is None
    vmem = pl.BlockSpec(memory_space=pltpu.VMEM)
    hbm = pl.BlockSpec(memory_space=pl.ANY)
    args = [meta, *gates, *qs, *kvs]
    specs = [pl.BlockSpec(memory_space=pltpu.SMEM)] + [vmem] * 6 + [hbm] * len(kvs)
    if not first:
        args += list(state)
        specs += [vmem, vmem]
    pair = (4, QG, 128)
    if last:
        out_shape = jax.ShapeDtypeStruct((16, 64, 128), BF)
        out_specs = vmem
    else:
        out_shape = [jax.ShapeDtypeStruct(pair, F32)] * 2
        out_specs = [vmem, vmem]
    scratch = [
        pltpu.VMEM((4096 * n_pairs, 128), BF),
        pltpu.VMEM((4, QG, 128), BF),
        pltpu.VMEM((128, 128), F32),
        pltpu.SemaphoreType.DMA((2 * n_pairs,)),
    ]
    if last:
        scratch += [pltpu.VMEM(pair, F32), pltpu.VMEM(pair, F32)]
    return pl.pallas_call(
        functools.partial(attend_kernel, n_pairs, first, last),
        in_specs=specs,
        out_shape=out_shape,
        out_specs=out_specs,
        scratch_shapes=scratch,
        name="attend",
    )(*args)


def rms_scale(rows, gain):
    mean_sq = jnp.mean(rows * rows, axis=-1, keepdims=True)
    return rows * lax.rsqrt(mean_sq + NORM_EPS) * gain


PITCH = 24


def slots_of(ids):
    expert = lax.broadcasted_iota(jnp.int32, (TILE, 128), 1)
    first = (ids[:, 0:1] == expert).astype(F32)
    second = (ids[:, 1:2] == expert).astype(F32)
    named = first + second
    r = lax.broadcasted_iota(jnp.int32, (TILE, TILE), 0)
    c = lax.broadcasted_iota(jnp.int32, (TILE, TILE), 1)
    before = jnp.where(c < r, 1.0, 0.0).astype(BF)
    rank = jnp.dot(before, named.astype(BF), preferred_element_type=F32)
    return first, second, named, rank


def mix_kernel(got, w_out, residual, gain_mix, gain_pre, ids, stream, outgoing, x, proj, normed, scr):
    lane = lax.broadcasted_iota(jnp.int32, (64, 128), 1) < 64
    for hp in range(8):
        even, odd = 2 * hp, 2 * hp + 1

        def block(h):
            return got[(h % 4) * 4 + h // 4].astype(F32)

        e, o = block(even), block(odd)
        cols = slice(hp * 128, hp * 128 + 128)
        x[0:64, cols] = jnp.where(lane, e, pltpu.roll(o, 64, 1)).astype(BF)
        x[64:128, cols] = jnp.where(lane, pltpu.roll(e, 64, 1), o).astype(BF)
    proj[...] = jnp.dot(x[...], w_out[...], preferred_element_type=F32)

    def norm(i, _):
        rows = pl.ds(pl.multiple_of(i * 16, 16), 16)
        mixed = residual[rows, :].astype(F32) + rms_scale(proj[rows, :], gain_mix[...])
        rounded = mixed.astype(BF)
        stream[rows, :] = rounded
        normed[rows, :] = rms_scale(rounded.astype(F32), gain_pre[...]).astype(BF)
        return 0

    lax.fori_loop(0, 8, norm, 0)

    _, _, named, rank = slots_of(ids[...])
    tn = (((0,), (0,)), ((), ()))
    for s in range(3):
        sel = jnp.where(rank == s, named, 0.0).astype(BF)
        for j in range(0, 16, 2):
            part = normed[:, j * 128 : j * 128 + 256]
            res = lax.dot_general(sel, part, tn, preferred_element_type=F32)
            scr[pl.ds(s * 128 * PITCH + j, 128, stride=PITCH), :] = res[:, 0:128]
            scr[pl.ds(s * 128 * PITCH + j + 1, 128, stride=PITCH), :] = res[:, 128:256]

    def put(e, _):
        for s in range(3):
            src = pl.multiple_of((s * 128 + e) * PITCH, 8)
            dst = pl.multiple_of(e * 48 + s * 16, 16)
            outgoing[pl.ds(dst, 16), :] = scr[pl.ds(src, 16), :].astype(BF)
        return 0

    lax.fori_loop(0, 128, put, 0, unroll=4)


def mix(got, w_out, residual, gain_mix, gain_pre, ids):
    vmem = pl.BlockSpec(memory_space=pltpu.VMEM)
    return pl.pallas_call(
        mix_kernel,
        in_specs=[vmem] * 6,
        out_shape=[jax.ShapeDtypeStruct((TILE, 2048), BF), jax.ShapeDtypeStruct((6144, 128), BF)],
        out_specs=[vmem, vmem],
        scratch_shapes=[
            pltpu.VMEM((TILE, 1024), BF),
            pltpu.VMEM((TILE, 2048), F32),
            pltpu.VMEM((TILE, 2048), BF),
            pltpu.VMEM((384 * PITCH, 128), F32),
        ],
        name="mix",
    )(got, w_out, residual, gain_mix.reshape(1, -1), gain_pre.reshape(1, -1), ids)


def expert_kernel(arrived, w_gate, w_up, w_down, out, scr, x):
    def take(r, _):
        src = pl.multiple_of(r * 16, 16)
        scr[pl.ds(pl.multiple_of(r * PITCH, 8), 16), :] = arrived[pl.ds(src, 16), :].astype(F32)
        return 0

    lax.fori_loop(0, 384, take, 0, unroll=8)
    for j in range(16):
        x[:, j * 128 : j * 128 + 128] = scr[pl.ds(j, 384, stride=PITCH), :].astype(BF)
    gate_act = jnp.dot(x[...], w_gate[0], preferred_element_type=F32)
    up_act = jnp.dot(x[...], w_up[0], preferred_element_type=F32)
    hidden = (jax.nn.silu(gate_act) * up_act).astype(BF)
    for j in range(0, 16, 2):
        res = jnp.dot(hidden, w_down[0, :, j * 128 : j * 128 + 256], preferred_element_type=F32)
        scr[pl.ds(j, 384, stride=PITCH), :] = res[:, 0:128]
        scr[pl.ds(j + 1, 384, stride=PITCH), :] = res[:, 128:256]

    def put(r, _):
        dst = pl.multiple_of(r * 16, 16)
        out[pl.ds(dst, 16), :] = scr[pl.ds(pl.multiple_of(r * PITCH, 8), 16), :].astype(BF)
        return 0

    lax.fori_loop(0, 384, put, 0, unroll=8)


def expert(arrived, w_gate, w_up, w_down):
    vmem = pl.BlockSpec(memory_space=pltpu.VMEM)
    return pl.pallas_call(
        expert_kernel,
        in_specs=[vmem] * 4,
        out_shape=jax.ShapeDtypeStruct((6144, 128), BF),
        out_specs=vmem,
        scratch_shapes=[pltpu.VMEM((384 * PITCH, 128), F32), pltpu.VMEM((384, 2048), BF)],
        name="expert",
    )(arrived, w_gate, w_up, w_down)


def combine_kernel(returned, stream, ids, weight, gain_post, out, scr, comb):
    def take(e, _):
        for s in range(3):
            src = pl.multiple_of(e * 48 + s * 16, 16)
            dst = pl.multiple_of((s * 128 + e) * PITCH, 8)
            scr[pl.ds(dst, 16), :] = returned[pl.ds(src, 16), :].astype(F32)
        return 0

    lax.fori_loop(0, 128, take, 0, unroll=4)
    first, second, _, rank = slots_of(ids[...])
    w = weight[...]
    share = first * w[:, 0:1] + second * w[:, 1:2]
    full = jnp.concatenate([jnp.where(rank == s, share, 0.0) for s in range(3)], axis=1)
    hi = full.astype(BF)
    rest = full - hi.astype(F32)
    mid = rest.astype(BF)
    low = (rest - mid.astype(F32)).astype(BF)
    for j in range(16):
        rows = scr[pl.ds(j, 384, stride=PITCH), :].astype(BF)
        res = jnp.dot(low, rows, preferred_element_type=F32)
        res += jnp.dot(mid, rows, preferred_element_type=F32)
        res += jnp.dot(hi, rows, preferred_element_type=F32)
        comb[:, j * 128 : j * 128 + 128] = res

    def norm(i, _):
        rows = pl.ds(pl.multiple_of(i * 16, 16), 16)
        out[rows, :] = (stream[rows, :].astype(F32) + rms_scale(comb[rows, :], gain_post[...])).astype(BF)
        return 0

    lax.fori_loop(0, 8, norm, 0)


def combine(returned, stream, ids, weight, gain_post):
    vmem = pl.BlockSpec(memory_space=pltpu.VMEM)
    return pl.pallas_call(
        combine_kernel,
        in_specs=[vmem] * 5,
        out_shape=jax.ShapeDtypeStruct((TILE, 2048), BF),
        out_specs=vmem,
        scratch_shapes=[pltpu.VMEM((384 * PITCH, 128), F32), pltpu.VMEM((TILE, 2048), F32)],
        name="combine",
    )(returned, stream, ids, weight, gain_post.reshape(1, -1))


def attention(queries, key_rows, value_rows, cum_gate):
    sp, tp = lax.axis_index("sp"), lax.axis_index("tp")
    z, x, core = sp // 4, sp % 4, tp % 2
    left, right, far = (x + 3) % 4, (x + 1) % 4, (x + 2) % 4
    gate_own = cum_gate.reshape(256, 128)
    gate_peer = lax.ppermute(gate_own, "tp", CORE_PAIRS)
    meta = jnp.stack([z, x, core, x, left, right, far]).astype(jnp.int32)
    msgs = pack(meta, queries, key_rows, value_rows)
    recv = [
        lax.ppermute(msgs[2 * m1 + m2], ALL, exchange_pairs(m1, m2))
        for m1 in range(2)
        for m2 in range(2)
    ]
    qs = [r[QG:] for r in recv]
    own = jnp.concatenate([r[:QG] for r in recv], axis=0)

    def swap(a):
        return lax.ppermute(a, "tp", CORE_PAIRS)

    from_left = lax.ppermute(own, "sp", ring_pairs(1))
    from_right = lax.ppermute(own, "sp", ring_pairs(-1))
    peer = swap(own)
    far_a = lax.ppermute(from_left[:1024], "sp", ring_pairs(1))
    far_b = lax.ppermute(from_right[1024:], "sp", ring_pairs(-1))
    left_peer, right_peer = swap(from_left), swap(from_right)
    far_own = jnp.concatenate([far_a, far_b], axis=0)
    far_peer = swap(far_own)
    out = attend(
        meta,
        (gate_own, gate_peer),
        qs,
        [own, peer, from_left, left_peer, from_right, right_peer, far_own, far_peer],
    )
    got = lax.all_to_all(out, ALL, split_axis=0, concat_axis=0, tiled=True, axis_index_groups=out_groups())
    return got


def local(
    queries,
    key_rows,
    value_rows,
    cum_gate,
    residual,
    out_weight,
    gain_mix,
    gain_pre,
    gain_post,
    route_ids,
    route_weight,
    w_gate,
    w_up,
    w_down,
):
    got = attention(queries, key_rows, value_rows, cum_gate)

    def exchange(rows):
        moved = lax.all_to_all(rows.reshape(128, 48, 128), ALL, split_axis=0, concat_axis=0, tiled=True)
        return moved.reshape(6144, 128)

    stream, outgoing = mix(got, out_weight, residual, gain_mix, gain_pre, route_ids)
    arrived = exchange(outgoing)
    returned = exchange(expert(arrived, w_gate, w_up, w_down))
    return combine(returned, stream, route_ids, route_weight, gain_post)


def solution(mesh):
    return jax.shard_map(
        local,
        mesh=mesh,
        in_specs=(
            P("sp", "tp"),
            P("sp", "tp"),
            P("sp", "tp"),
            P("tp", None),
            P(("sp", "tp"), None),
            P(),
            P(),
            P(),
            P(),
            P(("sp", "tp"), None),
            P(("sp", "tp"), None),
            P(("sp", "tp"), None, None),
            P(("sp", "tp"), None, None),
            P(("sp", "tp"), None, None),
        ),
        out_specs=P(("sp", "tp"), None),
        check_vma=False,
    )
```

```python
import functools

import jax
import jax.numpy as jnp
import numpy as np
from jax import lax
from jax.experimental import pallas as pl
from jax.experimental.pallas import tpu as pltpu
from jax.sharding import PartitionSpec as P

HEAD_DIM = 64
NORM_EPS = 1e-06
MASKED = -1e30
BF = jnp.bfloat16
F32 = jnp.float32
ALL = ("sp", "tp")
BLK = 1024
TILE = 128
QG = 512


def member(k, z):
    return 4 * z + (k if z % 2 == 0 else 3 - k)


def group_of(sp):
    z, x = divmod(sp, 4)
    return x if z % 2 == 0 else 3 - x


def exchange_pairs(m1, m2):
    pairs = []
    for sp in range(16):
        z = sp // 4
        for tp in range(8):
            y, s = divmod(tp, 2)
            to_z = 2 * s + (m1 ^ (z & 1))
            to_c = m2 ^ (z >> 1)
            pairs.append((sp * 8 + tp, member(group_of(sp), to_z) * 8 + 2 * y + to_c))
    return pairs


def ring_pairs(step):
    return [(sp, 4 * (sp // 4) + (sp % 4 + step) % 4) for sp in range(16)]


def out_groups():
    return [
        [member(k, z) * 8 + 2 * y + c for z in range(4) for y in range(4)]
        for k in range(4)
        for c in range(2)
    ]


CORE_PAIRS = [(i, i ^ 1) for i in range(8)]


def pack_kernel(meta, q_ref, k_ref, v_ref, *outs):
    z = meta[0, 0]
    row = lax.broadcasted_iota(jnp.int32, (128, 128), 0)
    col = lax.broadcasted_iota(jnp.int32, (128, 128), 1)

    def dot(a, b):
        return jnp.dot(a, b, preferred_element_type=F32)

    for m1 in range(2):
        f1 = m1 ^ (z & 1)
        low = jnp.where((col < 64) & (row == col + 64 * f1), 1.0, 0.0)
        high = jnp.where((col >= 64) & (row == col - 64 + 64 * f1), 1.0, 0.0)
        sel_lo, sel_hi = low.astype(BF), high.astype(BF)
        q_lo, q_hi = (low * 0.125).astype(BF), (high * 0.125).astype(BF)
        for i in range(4):
            even = q_ref[2 * i * TILE : (2 * i + 1) * TILE, :]
            odd = q_ref[(2 * i + 1) * TILE : (2 * i + 2) * TILE, :]
            qq = (dot(even, q_lo) + dot(odd, q_hi)).astype(BF)
            for m2 in range(2):
                outs[2 * m1 + m2][QG + i * TILE : QG + (i + 1) * TILE, :] = qq
        for m2 in range(2):
            f2 = m2 ^ (z >> 1)
            out = outs[2 * m1 + m2]
            for i in range(4):
                src = pl.ds(pl.multiple_of((2 * i + f2) * TILE, TILE), TILE)
                kv = dot(k_ref[src, :], sel_lo) + dot(v_ref[src, :], sel_hi)
                out[i * TILE : (i + 1) * TILE, :] = kv.astype(BF)


def pack(meta, q, k, v):
    return pl.pallas_call(
        pack_kernel,
        in_specs=[pl.BlockSpec(memory_space=pltpu.SMEM)] + [pl.BlockSpec(memory_space=pltpu.VMEM)] * 3,
        out_shape=[jax.ShapeDtypeStruct((BLK, 128), BF)] * 4,
        out_specs=[pl.BlockSpec(memory_space=pltpu.VMEM)] * 4,
        name="pack",
        compiler_params=pltpu.CompilerParams(vmem_limit_bytes=8 * 2**20),
    )(meta, q, k, v)


ROWS_STEP = 1024
FR, FK, AHEAD, UNROLL = 512, 256, 1, 2
HUGE = 1e30
CALLS = (1, 2, 1)
STEP0 = (16, 72, 144)


def block_of(z, core, slot, x_of):
    zb = ((slot // 2) ^ (z & 1)) + 2 * ((slot % 2) ^ core)
    return zb, 4 * zb + (3 - x_of if slot // 2 else x_of)


def device_table():
    table = np.zeros((128, 256), np.int32)
    for sp in range(16):
        z, x = divmod(sp, 4)
        for core in range(2):
            row = np.zeros(256, np.int32)
            row[0:3] = z, x, core
            zq = [block_of(z, core, g, x)[0] for g in range(4)]
            row[4:8] = zq
            for call, chunks in enumerate(((x,), ((x + 3) % 4, (x + 1) % 4), ((x + 2) % 4,))):
                steps = []
                for i, x_of in enumerate(chunks):
                    for g in range(4):
                        for slot in range(4):
                            b_q, b_k = block_of(z, core, g, x)[1], block_of(z, core, slot, x_of)[1]
                            if b_k < b_q:
                                steps.append((g, i * 2048 + slot * QG, b_k * 8, b_q * 8))
                assert len(steps) == (6, 16, 8)[call]
                flat = np.array(steps + [(0, 0, 0, 0)] * 2, np.int32).reshape(-1)
                row[STEP0[call] : STEP0[call] + len(flat)] = flat
            for y in range(4):
                table[sp * 8 + 2 * y + core] = row
    return table


NT = (((1,), (1,)), ((), ()))


def attend_kernel(call, first, last, table, *refs):
    refs = list(refs)
    n = CALLS[call]
    if first:
        gate_own, gate_peer = refs.pop(0), refs.pop(0)
        qs = [refs.pop(0) for _ in range(4)]
    else:
        gate, q_pad, m_in, acc_in = [refs.pop(0) for _ in range(4)]
    kv_in = [refs.pop(0) for _ in range(n)]
    if first:
        gate, q_pad, m_ref, acc_ref = [refs.pop(0) for _ in range(4)]
    elif last:
        keep_ref, send_ref = refs.pop(0), refs.pop(0)
    else:
        m_ref, acc_ref = refs.pop(0), refs.pop(0)
    kv, sems = refs.pop(0), refs.pop(0)
    if last:
        m_ref, acc_ref = refs.pop(0), refs.pop(0)
    z, core = table[0, 0], table[0, 2]

    copies = [pltpu.make_async_copy(src, kv.at[pl.ds(i * 2048, 2048)], sems.at[i]) for i, src in enumerate(kv_in)]
    for c in copies:
        c.start()
    if first:
        mine = lax.shift_right_logical(z, 1) == core
        row0 = pl.multiple_of((z & 1) * 128, 128)
        gate[...] = jnp.where(mine, gate_own[pl.ds(row0, 128), :], gate_peer[pl.ds(row0, 128), :])
        lane = lax.broadcasted_iota(jnp.int32, (QG, 128), 1)
        for g in range(4):
            packed = qs[g][QG:, :].astype(F32)
            q_pad[g, 0:QG, :] = jnp.where(lane < 64, packed, 0.0).astype(BF)
            q_pad[g, QG:, :] = jnp.where(lane < 64, pltpu.roll(packed, 64, 1), 0.0).astype(BF)
    else:
        acc_ref[...] = acc_in[...]
        m_ref[...] = m_in[...]
    for c in copies:
        c.wait()

    def operands(start, key_gate, query_gate):
        keys = kv[pl.ds(pl.multiple_of(start, QG), QG), :]
        parts = [gate[pl.ds(key_gate + 2 * i + core, 1), :] for i in range(4)]
        shift = jnp.concatenate(parts, axis=1) - gate[pl.ds(query_gate, 1), 0:1]
        ones = lax.broadcasted_iota(jnp.int32, (QG, 128), 1) < 64
        return keys, jnp.where(ones, jnp.ones_like(keys), keys), shift

    def spread(rows):
        return jnp.concatenate([rows] * (FK // 128), axis=1)

    def diagonal(g):
        block = 4 * table[0, 4 + g] * 8 + xb_of(g) * 8
        keys, values, shift = operands(g * QG, block, block)
        r = lax.broadcasted_iota(jnp.int32, (TILE, TILE), 0)
        cc = lax.broadcasted_iota(jnp.int32, (TILE, TILE), 1)
        tri = jnp.where(cc <= r, 0.0, MASKED)
        even = jnp.where(core == 0, tri, jnp.full_like(tri, MASKED))
        odd = jnp.where(core == 0, jnp.zeros_like(tri), tri)
        edge = jnp.concatenate([even, odd], axis=0)
        for i in range(4):
            lo, hi = slice(i * TILE, (i + 1) * TILE), slice(QG + i * TILE, QG + (i + 1) * TILE)
            q = jnp.concatenate([q_pad[g, lo, :], q_pad[g, hi, :]], axis=0)
            width = (i + 1) * TILE
            s = lax.dot_general(q, keys[0:width], NT, preferred_element_type=F32) - shift[:, 0:width]
            raw = s[:, width - TILE :]
            s_edge = raw + edge
            top = jnp.max(s_edge, axis=1, keepdims=True)
            if i == 0:
                level = -4.0 * jnp.sum(jnp.abs(q.astype(F32)), axis=1, keepdims=True)
                top = jnp.where(top <= 0.1 * MASKED, level, top)
                p = jnp.exp(s_edge - top).astype(BF)
            else:
                body = s[:, 0 : width - TILE]
                top = jnp.maximum(top, jnp.max(body, axis=1, keepdims=True))
                p = jnp.exp(jnp.concatenate([body, s_edge], axis=1) - top).astype(BF)
            pv = jnp.dot(p, values[0:width], preferred_element_type=F32)
            top = jnp.broadcast_to(top, (2 * TILE, 128))
            acc_ref[g, lo, :], acc_ref[g, hi, :] = pv[0:TILE], pv[TILE:]
            m_ref[g, lo, :], m_ref[g, hi, :] = top[0:TILE], top[TILE:]

    def xb_of(g):
        return jnp.where(g // 2 == 1, 3 - table[0, 1], table[0, 1])

    def step_operands(t):
        at = STEP0[call] + 4 * t
        return table[0, at], operands(table[0, at + 1], table[0, at + 2], table[0, at + 3])

    def fast(t):
        g, (keys, values, shift) = step_operands(t)
        units = [(r0, k0) for r0 in range(0, ROWS_STEP, FR) for k0 in range(0, QG, FK)]

        def qk(r0, k0):
            return lax.dot_general(q_pad[g, r0 : r0 + FR, :], keys[k0 : k0 + FK], NT, preferred_element_type=F32)

        ahead = [qk(*units[i]) for i in range(AHEAD)]
        pv = None
        for u, (r0, k0) in enumerate(units):
            s = ahead.pop(0)
            if u + AHEAD < len(units):
                ahead.append(qk(*units[u + AHEAD]))
            m_rows = spread(m_ref[g, r0 : r0 + FR, :])
            p = jnp.exp(s - shift[:, k0 : k0 + FK] - m_rows).astype(BF)
            part = jnp.dot(p, values[k0 : k0 + FK], preferred_element_type=F32)
            pv = part if k0 == 0 else pv + part
            if k0 + FK == QG:
                acc_ref[g, r0 : r0 + FR, :] += pv

    def careful(t):
        g, (keys, values, shift) = step_operands(t)

        def some(i, _):
            rows = pl.ds(pl.multiple_of(i * 256, 256), 256)
            s = lax.dot_general(q_pad[g, rows, :], keys, NT, preferred_element_type=F32) - shift
            m_old = m_ref[g, rows, :]
            m_new = jnp.maximum(m_old, jnp.max(s, axis=1, keepdims=True))
            p = jnp.exp(s - m_new[:, 0:1]).astype(BF)
            pv = jnp.dot(p, values, preferred_element_type=F32)
            acc_ref[g, rows, :] = acc_ref[g, rows, :] * jnp.exp(m_old - m_new) + pv
            m_ref[g, rows, :] = m_new
            return 0

        lax.fori_loop(0, 4, some, 0)

    if first:

        def start(g, _):
            diagonal(g)
            return 0

        lax.fori_loop(0, 4, start, 0)

    steps = (6, 16, 8)[call]

    def body(i, _):
        for u in range(UNROLL):
            fast(UNROLL * i + u)
        return 0

    lax.fori_loop(0, steps // UNROLL, body, 0)

    def look(g, bad):
        lane = lax.broadcasted_iota(jnp.int32, (ROWS_STEP, 128), 1)
        return bad + jnp.where((acc_ref[g] <= HUGE) | (lane > 0), 0.0, 1.0)

    bad = lax.fori_loop(0, 4, look, jnp.zeros((ROWS_STEP, 128), F32))

    @pl.when(jnp.max(bad) > 0.0)
    def _():
        if first:

            def restart(g, _):
                diagonal(g)
                return 0

            lax.fori_loop(0, 4, restart, 0)
        else:

            def restore(g, _):
                acc_ref[g] = acc_in[g]
                m_ref[g] = m_in[g]
                return 0

            lax.fori_loop(0, 4, restore, 0)

        def again(t, _):
            careful(t)
            return 0

        lax.fori_loop(0, steps, again, 0)

    if last:

        def finish(g, _):
            zq = table[0, 4 + g]
            lane = lax.broadcasted_iota(jnp.int32, (QG, 128), 1)
            for half, ref in ((core, keep_ref), (1 - core, send_ref)):
                rows = pl.ds(pl.multiple_of(half * QG, QG), QG)
                ref[zq] = jnp.where(lane == 0, m_ref[g, rows, :], acc_ref[g, rows, :])
            return 0

        lax.fori_loop(0, 4, finish, 0)


def attend(call, table, shared, kvs, state=None):
    n = CALLS[call]
    first, last = call == 0, call == 2
    vmem = pl.BlockSpec(memory_space=pltpu.VMEM)
    hbm = pl.BlockSpec(memory_space=pl.ANY)
    args = [table, *shared] + list(state or ()) + list(kvs)
    specs = [pl.BlockSpec(memory_space=pltpu.SMEM)] + [vmem] * (len(args) - 1 - n) + [hbm] * n
    pair = (4, ROWS_STEP, 128)
    if last:
        out_shape = [jax.ShapeDtypeStruct((4, QG, 128), F32)] * 2
    else:
        out_shape = [pltpu.VMEM(pair, F32)] * 2
    if first:
        out_shape = [pltpu.VMEM((128, 128), F32), pltpu.VMEM(pair, BF)] + out_shape
    scratch = [pltpu.VMEM((2048 * n, 128), BF), pltpu.SemaphoreType.DMA((n,))]
    if last:
        scratch += [pltpu.VMEM(pair, F32), pltpu.VMEM(pair, F32)]
    steps = (9, 16, 8)[call]
    return pl.pallas_call(
        functools.partial(attend_kernel, call, first, last),
        in_specs=specs,
        out_shape=out_shape,
        out_specs=[vmem] * len(out_shape),
        scratch_shapes=scratch,
        cost_estimate=pl.CostEstimate(
            flops=steps * ROWS_STEP * QG * 512 * 2,
            transcendentals=steps * ROWS_STEP * QG,
            bytes_accessed=n * 2048 * 256,
        ),
        name="attend",
        compiler_params=pltpu.CompilerParams(vmem_limit_bytes=22 * 2**20),
    )(*args)


def merge_kernel(keep, other, out_ref):
    lane64 = lax.broadcasted_iota(jnp.int32, (64, 128), 1) < 64
    for zq in range(4):
        for i in range(4):
            rows = slice(i * TILE, (i + 1) * TILE)
            a, b = keep[zq, rows, :], other[zq, rows, :]
            m_a, m_b = a[:, 0:1], b[:, 0:1]
            top = jnp.maximum(m_a, m_b)
            w_a, w_b = jnp.exp(m_a - top), jnp.exp(m_b - top)
            total = a[:, 1:2] * w_a + b[:, 1:2] * w_b
            o = a * (w_a / total) + b * (w_b / total)
            packed = jnp.where(lane64, pltpu.roll(o[0:64], 64, 1), o[64:128])
            out_ref[zq * 4 + i, :, :] = packed.astype(BF)


def merge(keep, other):
    vmem = pl.BlockSpec(memory_space=pltpu.VMEM)
    return pl.pallas_call(
        merge_kernel,
        in_specs=[vmem, vmem],
        out_shape=jax.ShapeDtypeStruct((16, 64, 128), BF),
        out_specs=vmem,
        name="merge",
        compiler_params=pltpu.CompilerParams(vmem_limit_bytes=12 * 2**20),
    )(keep, other)


def rms_scale(rows, gain):
    mean_sq = jnp.mean(rows * rows, axis=-1, keepdims=True)
    return rows * lax.rsqrt(mean_sq + NORM_EPS) * gain


PITCH = 24


def slots_of(ids):
    expert = lax.broadcasted_iota(jnp.int32, (TILE, 128), 1)
    first = (ids[:, 0:1] == expert).astype(F32)
    second = (ids[:, 1:2] == expert).astype(F32)
    named = first + second
    r = lax.broadcasted_iota(jnp.int32, (TILE, TILE), 0)
    c = lax.broadcasted_iota(jnp.int32, (TILE, TILE), 1)
    before = jnp.where(c < r, 1.0, 0.0).astype(BF)
    rank = jnp.dot(before, named.astype(BF), preferred_element_type=F32)
    return first, second, named, rank


def mix_kernel(got, w_out, residual, gain_mix, gain_pre, ids, stream, outgoing, x, proj, normed, scr):
    lane = lax.broadcasted_iota(jnp.int32, (64, 128), 1) < 64
    for hp in range(8):
        even, odd = 2 * hp, 2 * hp + 1

        def block(h):
            return got[(h % 4) * 4 + h // 4].astype(F32)

        e, o = block(even), block(odd)
        cols = slice(hp * 128, hp * 128 + 128)
        x[0:64, cols] = jnp.where(lane, e, pltpu.roll(o, 64, 1)).astype(BF)
        x[64:128, cols] = jnp.where(lane, pltpu.roll(e, 64, 1), o).astype(BF)
    proj[...] = jnp.dot(x[...], w_out[...], preferred_element_type=F32)

    def norm(i, _):
        rows = pl.ds(pl.multiple_of(i * 16, 16), 16)
        mixed = residual[rows, :].astype(F32) + rms_scale(proj[rows, :], gain_mix[...])
        rounded = mixed.astype(BF)
        stream[rows, :] = rounded
        normed[rows, :] = rms_scale(rounded.astype(F32), gain_pre[...]).astype(BF)
        return 0

    lax.fori_loop(0, 8, norm, 0)

    _, _, named, rank = slots_of(ids[...])
    tn = (((0,), (0,)), ((), ()))
    for s in range(3):
        sel = jnp.where(rank == s, named, 0.0).astype(BF)
        for j in range(0, 16, 2):
            part = normed[:, j * 128 : j * 128 + 256]
            res = lax.dot_general(sel, part, tn, preferred_element_type=F32)
            scr[pl.ds(s * 128 * PITCH + j, 128, stride=PITCH), :] = res[:, 0:128]
            scr[pl.ds(s * 128 * PITCH + j + 1, 128, stride=PITCH), :] = res[:, 128:256]

    def put(e, _):
        for s in range(3):
            src = pl.multiple_of((s * 128 + e) * PITCH, 8)
            dst = pl.multiple_of(e * 48 + s * 16, 16)
            outgoing[pl.ds(dst, 16), :] = scr[pl.ds(src, 16), :].astype(BF)
        return 0

    lax.fori_loop(0, 128, put, 0, unroll=4)


def mix(got, w_out, residual, gain_mix, gain_pre, ids):
    vmem = pl.BlockSpec(memory_space=pltpu.VMEM)
    return pl.pallas_call(
        mix_kernel,
        in_specs=[vmem] * 6,
        out_shape=[jax.ShapeDtypeStruct((TILE, 2048), BF), jax.ShapeDtypeStruct((6144, 128), BF)],
        out_specs=[vmem, vmem],
        scratch_shapes=[
            pltpu.VMEM((TILE, 1024), BF),
            pltpu.VMEM((TILE, 2048), F32),
            pltpu.VMEM((TILE, 2048), BF),
            pltpu.VMEM((384 * PITCH, 128), F32),
        ],
        name="mix",
        compiler_params=pltpu.CompilerParams(vmem_limit_bytes=24 * 2**20),
    )(got, w_out, residual, gain_mix.reshape(1, -1), gain_pre.reshape(1, -1), ids)


def expert_kernel(arrived, w_gate, w_up, w_down, out, scr, x):
    def take(r, _):
        src = pl.multiple_of(r * 16, 16)
        scr[pl.ds(pl.multiple_of(r * PITCH, 8), 16), :] = arrived[pl.ds(src, 16), :].astype(F32)
        return 0

    lax.fori_loop(0, 384, take, 0, unroll=8)
    for j in range(16):
        x[:, j * 128 : j * 128 + 128] = scr[pl.ds(j, 384, stride=PITCH), :].astype(BF)
    gate_act = jnp.dot(x[...], w_gate[0], preferred_element_type=F32)
    up_act = jnp.dot(x[...], w_up[0], preferred_element_type=F32)
    hidden = (jax.nn.silu(gate_act) * up_act).astype(BF)
    for j in range(0, 16, 2):
        res = jnp.dot(hidden, w_down[0, :, j * 128 : j * 128 + 256], preferred_element_type=F32)
        scr[pl.ds(j, 384, stride=PITCH), :] = res[:, 0:128]
        scr[pl.ds(j + 1, 384, stride=PITCH), :] = res[:, 128:256]

    def put(r, _):
        dst = pl.multiple_of(r * 16, 16)
        out[pl.ds(dst, 16), :] = scr[pl.ds(pl.multiple_of(r * PITCH, 8), 16), :].astype(BF)
        return 0

    lax.fori_loop(0, 384, put, 0, unroll=8)


def expert(arrived, w_gate, w_up, w_down):
    vmem = pl.BlockSpec(memory_space=pltpu.VMEM)
    return pl.pallas_call(
        expert_kernel,
        in_specs=[vmem] * 4,
        out_shape=jax.ShapeDtypeStruct((6144, 128), BF),
        out_specs=vmem,
        scratch_shapes=[pltpu.VMEM((384 * PITCH, 128), F32), pltpu.VMEM((384, 2048), BF)],
        name="expert",
        compiler_params=pltpu.CompilerParams(vmem_limit_bytes=26 * 2**20),
    )(arrived, w_gate, w_up, w_down)


def combine_kernel(returned, stream, ids, weight, gain_post, out, scr, comb):
    def take(e, _):
        for s in range(3):
            src = pl.multiple_of(e * 48 + s * 16, 16)
            dst = pl.multiple_of((s * 128 + e) * PITCH, 8)
            scr[pl.ds(dst, 16), :] = returned[pl.ds(src, 16), :].astype(F32)
        return 0

    lax.fori_loop(0, 128, take, 0, unroll=4)
    first, second, _, rank = slots_of(ids[...])
    w = weight[...]
    share = first * w[:, 0:1] + second * w[:, 1:2]
    full = jnp.concatenate([jnp.where(rank == s, share, 0.0) for s in range(3)], axis=1)
    hi = full.astype(BF)
    rest = full - hi.astype(F32)
    mid = rest.astype(BF)
    low = (rest - mid.astype(F32)).astype(BF)
    for j in range(16):
        rows = scr[pl.ds(j, 384, stride=PITCH), :].astype(BF)
        res = jnp.dot(low, rows, preferred_element_type=F32)
        res += jnp.dot(mid, rows, preferred_element_type=F32)
        res += jnp.dot(hi, rows, preferred_element_type=F32)
        comb[:, j * 128 : j * 128 + 128] = res

    def norm(i, _):
        rows = pl.ds(pl.multiple_of(i * 16, 16), 16)
        out[rows, :] = (stream[rows, :].astype(F32) + rms_scale(comb[rows, :], gain_post[...])).astype(BF)
        return 0

    lax.fori_loop(0, 8, norm, 0)


def combine(returned, stream, ids, weight, gain_post):
    vmem = pl.BlockSpec(memory_space=pltpu.VMEM)
    return pl.pallas_call(
        combine_kernel,
        in_specs=[vmem] * 5,
        out_shape=jax.ShapeDtypeStruct((TILE, 2048), BF),
        out_specs=vmem,
        scratch_shapes=[pltpu.VMEM((384 * PITCH, 128), F32), pltpu.VMEM((TILE, 2048), F32)],
        name="combine",
        compiler_params=pltpu.CompilerParams(vmem_limit_bytes=16 * 2**20),
    )(returned, stream, ids, weight, gain_post.reshape(1, -1))


def attention(queries, key_rows, value_rows, cum_gate):
    device = lax.axis_index("sp") * 8 + lax.axis_index("tp")
    table = lax.dynamic_slice_in_dim(jnp.asarray(device_table()), device, 1, 0)
    gate_own = cum_gate.reshape(256, 128)
    gate_peer = lax.ppermute(gate_own, "tp", CORE_PAIRS)
    msgs = pack(table, queries, key_rows, value_rows)
    recv = [
        lax.ppermute(msgs[2 * m1 + m2], ALL, exchange_pairs(m1, m2))
        for m1 in range(2)
        for m2 in range(2)
    ]
    own = jnp.concatenate([r[:QG] for r in recv], axis=0)
    from_left = lax.ppermute(own, "sp", ring_pairs(1))
    from_right = lax.ppermute(own, "sp", ring_pairs(-1))
    far_a = lax.ppermute(from_left[:1024], "sp", ring_pairs(1))
    far_b = lax.ppermute(from_right[1024:], "sp", ring_pairs(-1))
    gate, q_pad, *state = attend(0, table, (gate_own, gate_peer, *recv), [own])
    state = attend(1, table, (gate, q_pad), [from_left, from_right], state)
    far_own = jnp.concatenate([far_a, far_b], axis=0)
    keep, send = attend(2, table, (gate, q_pad), [far_own], state)
    out = merge(keep, lax.ppermute(send, "tp", CORE_PAIRS))
    return lax.all_to_all(out, ALL, split_axis=0, concat_axis=0, tiled=True, axis_index_groups=out_groups())


def local(
    queries,
    key_rows,
    value_rows,
    cum_gate,
    residual,
    out_weight,
    gain_mix,
    gain_pre,
    gain_post,
    route_ids,
    route_weight,
    w_gate,
    w_up,
    w_down,
):
    got = attention(queries, key_rows, value_rows, cum_gate)

    def exchange(rows):
        moved = lax.all_to_all(rows.reshape(128, 48, 128), ALL, split_axis=0, concat_axis=0, tiled=True)
        return moved.reshape(6144, 128)

    stream, outgoing = mix(got, out_weight, residual, gain_mix, gain_pre, route_ids)
    arrived = exchange(outgoing)
    returned = exchange(expert(arrived, w_gate, w_up, w_down))
    return combine(returned, stream, route_ids, route_weight, gain_post)


def solution(mesh):
    return jax.shard_map(
        local,
        mesh=mesh,
        in_specs=(
            P("sp", "tp"),
            P("sp", "tp"),
            P("sp", "tp"),
            P("tp", None),
            P(("sp", "tp"), None),
            P(),
            P(),
            P(),
            P(),
            P(("sp", "tp"), None),
            P(("sp", "tp"), None),
            P(("sp", "tp"), None, None),
            P(("sp", "tp"), None, None),
            P(("sp", "tp"), None, None),
        ),
        out_specs=P(("sp", "tp"), None),
        check_vma=False,
    )
```

```python
import functools

import jax
import jax.numpy as jnp
import numpy as np
from jax import lax
from jax.experimental import pallas as pl
from jax.experimental.pallas import tpu as pltpu
from jax.sharding import PartitionSpec as P

HEAD_DIM = 64
NORM_EPS = 1e-06
MASKED = -1e30
BF = jnp.bfloat16
F32 = jnp.float32
ALL = ("sp", "tp")
BLK = 1024
TILE = 128
QG = 512


def member(k, z):
    return 4 * z + (k if z % 2 == 0 else 3 - k)


def group_of(sp):
    z, x = divmod(sp, 4)
    return x if z % 2 == 0 else 3 - x


def exchange_pairs(m1, m2):
    pairs = []
    for sp in range(16):
        z = sp // 4
        for tp in range(8):
            y, s = divmod(tp, 2)
            to_z = 2 * s + (m1 ^ (z & 1))
            to_c = m2 ^ (z >> 1)
            pairs.append((sp * 8 + tp, member(group_of(sp), to_z) * 8 + 2 * y + to_c))
    return pairs


def ring_pairs(step):
    return [(sp, 4 * (sp // 4) + (sp % 4 + step) % 4) for sp in range(16)]


def out_groups():
    return [
        [member(k, z) * 8 + 2 * y + c for z in range(4) for y in range(4)]
        for k in range(4)
        for c in range(2)
    ]


CORE_PAIRS = [(i, i ^ 1) for i in range(8)]


def pack_kernel(q_in, k_in, v_in, *refs):
    outs, (q_ref, k_ref, v_ref, sems) = refs[:4], refs[4:]
    copies = [
        pltpu.make_async_copy(src, dst, sems.at[i])
        for i, (src, dst) in enumerate(((q_in, q_ref), (k_in, k_ref), (v_in, v_ref)))
    ]
    for c in copies:
        c.start()
    z = lax.axis_index("sp") // 4
    row = lax.broadcasted_iota(jnp.int32, (128, 128), 0)
    col = lax.broadcasted_iota(jnp.int32, (128, 128), 1)

    def dot(a, b):
        return jnp.dot(a, b, preferred_element_type=F32)

    for c in copies:
        c.wait()
    for m1 in range(2):
        f1 = m1 ^ (z & 1)
        low = jnp.where((col < 64) & (row == col + 64 * f1), 1.0, 0.0)
        high = jnp.where((col >= 64) & (row == col - 64 + 64 * f1), 1.0, 0.0)
        sel_lo, sel_hi = low.astype(BF), high.astype(BF)
        q_lo, q_hi = (low * 0.125).astype(BF), (high * 0.125).astype(BF)
        for i in range(4):
            even = q_ref[2 * i * TILE : (2 * i + 1) * TILE, :]
            odd = q_ref[(2 * i + 1) * TILE : (2 * i + 2) * TILE, :]
            qq = (dot(even, q_lo) + dot(odd, q_hi)).astype(BF)
            for m2 in range(2):
                outs[2 * m1 + m2][QG + i * TILE : QG + (i + 1) * TILE, :] = qq
        for m2 in range(2):
            f2 = m2 ^ (z >> 1)
            out = outs[2 * m1 + m2]
            for i in range(4):
                src = pl.ds(pl.multiple_of((2 * i + f2) * TILE, TILE), TILE)
                kv = dot(k_ref[src, :], sel_lo) + dot(v_ref[src, :], sel_hi)
                out[i * TILE : (i + 1) * TILE, :] = kv.astype(BF)


def pack(q, k, v):
    return pl.pallas_call(
        pack_kernel,
        in_specs=[pl.BlockSpec(memory_space=pltpu.HBM)] * 3,
        out_shape=[pltpu.VMEM((BLK, 128), BF)] * 4,
        out_specs=[pl.BlockSpec(memory_space=pltpu.VMEM)] * 4,
        scratch_shapes=[pltpu.VMEM((BLK, 128), BF)] * 3 + [pltpu.SemaphoreType.DMA((3,))],
        name="pack",
        compiler_params=pltpu.CompilerParams(vmem_limit_bytes=8 * 2**20),
    )(*(pltpu.with_memory_space_constraint(a, pltpu.HBM) for a in (q, k, v)))


ROWS_STEP = 1024
FR, FK, AHEAD = 512, 256, 1
UNROLL = (2, 4, 4)
HUGE = 1e30
CALLS = (1, 2, 1)
STEP0 = (16, 72, 144)


def block_of(z, core, slot, x_of):
    zb = ((slot // 2) ^ (z & 1)) + 2 * ((slot % 2) ^ core)
    return zb, 4 * zb + (3 - x_of if slot // 2 else x_of)


def device_table():
    table = np.zeros((128, 256), np.int32)
    for sp in range(16):
        z, x = divmod(sp, 4)
        for core in range(2):
            row = np.zeros(256, np.int32)
            row[0:3] = z, x, core
            zq = [block_of(z, core, g, x)[0] for g in range(4)]
            row[4:8] = zq
            for call, chunks in enumerate(((x,), ((x + 3) % 4, (x + 1) % 4), ((x + 2) % 4,))):
                steps = []
                for i, x_of in enumerate(chunks):
                    for g in range(4):
                        for slot in range(4):
                            b_q, b_k = block_of(z, core, g, x)[1], block_of(z, core, slot, x_of)[1]
                            if b_k < b_q:
                                steps.append((g, i * 2048 + slot * QG, b_k * 8, b_q * 8))
                assert len(steps) == (6, 16, 8)[call]
                flat = np.array(steps + [(0, 0, 0, 0)] * 2, np.int32).reshape(-1)
                row[STEP0[call] : STEP0[call] + len(flat)] = flat
            for y in range(4):
                table[sp * 8 + 2 * y + core] = row
    return table


NT = (((1,), (1,)), ((), ()))


def attend_kernel(call, first, last, table, *refs):
    refs = list(refs)
    n = CALLS[call]
    if first:
        gate_own, gate_peer = refs.pop(0), refs.pop(0)
        qs = [refs.pop(0) for _ in range(4)]
    else:
        gate, q_pad, m_in, acc_in = [refs.pop(0) for _ in range(4)]
    kv_in = [refs.pop(0) for _ in range(n)]
    if first:
        gate, q_pad, m_ref, acc_ref = [refs.pop(0) for _ in range(4)]
    elif last:
        keep_ref, send_ref = refs.pop(0), refs.pop(0)
    else:
        m_ref, acc_ref = refs.pop(0), refs.pop(0)
    kv, sems = refs.pop(0), refs.pop(0)
    if last:
        m_ref, acc_ref = refs.pop(0), refs.pop(0)
    z, core = table[0, 0], table[0, 2]

    copies = [pltpu.make_async_copy(src, kv.at[pl.ds(i * 2048, 2048)], sems.at[i]) for i, src in enumerate(kv_in)]
    for c in copies:
        c.start()
    if first:
        mine = lax.shift_right_logical(z, 1) == core
        row0 = pl.multiple_of((z & 1) * 128, 128)
        gate[...] = jnp.where(mine, gate_own[pl.ds(row0, 128), :], gate_peer[pl.ds(row0, 128), :])
        lane = lax.broadcasted_iota(jnp.int32, (QG, 128), 1)
        for g in range(4):
            packed = qs[g][QG:, :].astype(F32)
            q_pad[g, 0:QG, :] = jnp.where(lane < 64, packed, 0.0).astype(BF)
            q_pad[g, QG:, :] = jnp.where(lane < 64, pltpu.roll(packed, 64, 1), 0.0).astype(BF)
    else:
        acc_ref[...] = acc_in[...]
        m_ref[...] = m_in[...]
    for c in copies:
        c.wait()

    def operands(start, key_gate, query_gate):
        keys = kv[pl.ds(pl.multiple_of(start, QG), QG), :]
        parts = [gate[pl.ds(key_gate + 2 * i + core, 1), :] for i in range(4)]
        shift = jnp.concatenate(parts, axis=1) - gate[pl.ds(query_gate, 1), 0:1]
        ones = lax.broadcasted_iota(jnp.int32, (QG, 128), 1) < 64
        return keys, jnp.where(ones, jnp.ones_like(keys), keys), shift

    def spread(rows):
        return jnp.concatenate([rows] * (FK // 128), axis=1)

    def diagonal(g):
        block = 4 * table[0, 4 + g] * 8 + xb_of(g) * 8
        keys, values, shift = operands(g * QG, block, block)
        r = lax.broadcasted_iota(jnp.int32, (TILE, TILE), 0)
        cc = lax.broadcasted_iota(jnp.int32, (TILE, TILE), 1)
        tri = jnp.where(cc <= r, 0.0, MASKED)
        even = jnp.where(core == 0, tri, jnp.full_like(tri, MASKED))
        odd = jnp.where(core == 0, jnp.zeros_like(tri), tri)
        edge = jnp.concatenate([even, odd], axis=0)
        for i in range(4):
            lo, hi = slice(i * TILE, (i + 1) * TILE), slice(QG + i * TILE, QG + (i + 1) * TILE)
            q = jnp.concatenate([q_pad[g, lo, :], q_pad[g, hi, :]], axis=0)
            width = (i + 1) * TILE
            s = lax.dot_general(q, keys[0:width], NT, preferred_element_type=F32) - shift[:, 0:width]
            raw = s[:, width - TILE :]
            s_edge = raw + edge
            top = jnp.max(s_edge, axis=1, keepdims=True)
            if i == 0:
                level = -4.0 * jnp.sum(jnp.abs(q.astype(F32)), axis=1, keepdims=True)
                top = jnp.where(top <= 0.1 * MASKED, level, top)
                p = jnp.exp(s_edge - top).astype(BF)
            else:
                body = s[:, 0 : width - TILE]
                top = jnp.maximum(top, jnp.max(body, axis=1, keepdims=True))
                p = jnp.exp(jnp.concatenate([body, s_edge], axis=1) - top).astype(BF)
            pv = jnp.dot(p, values[0:width], preferred_element_type=F32)
            top = jnp.broadcast_to(top, (2 * TILE, 128))
            acc_ref[g, lo, :], acc_ref[g, hi, :] = pv[0:TILE], pv[TILE:]
            m_ref[g, lo, :], m_ref[g, hi, :] = top[0:TILE], top[TILE:]

    def xb_of(g):
        return jnp.where(g // 2 == 1, 3 - table[0, 1], table[0, 1])

    def step_operands(t):
        at = STEP0[call] + 4 * t
        return table[0, at], operands(table[0, at + 1], table[0, at + 2], table[0, at + 3])

    def fast(t):
        g, (keys, values, shift) = step_operands(t)
        units = [(r0, k0) for r0 in range(0, ROWS_STEP, FR) for k0 in range(0, QG, FK)]

        def qk(r0, k0):
            return lax.dot_general(q_pad[g, r0 : r0 + FR, :], keys[k0 : k0 + FK], NT, preferred_element_type=F32)

        ahead = [qk(*units[i]) for i in range(AHEAD)]
        pv = None
        for u, (r0, k0) in enumerate(units):
            s = ahead.pop(0)
            if u + AHEAD < len(units):
                ahead.append(qk(*units[u + AHEAD]))
            m_rows = spread(m_ref[g, r0 : r0 + FR, :])
            p = jnp.exp(s - shift[:, k0 : k0 + FK] - m_rows).astype(BF)
            part = jnp.dot(p, values[k0 : k0 + FK], preferred_element_type=F32)
            pv = part if k0 == 0 else pv + part
            if k0 + FK == QG:
                acc_ref[g, r0 : r0 + FR, :] += pv

    def careful(t):
        g, (keys, values, shift) = step_operands(t)

        def some(i, _):
            rows = pl.ds(pl.multiple_of(i * 256, 256), 256)
            s = lax.dot_general(q_pad[g, rows, :], keys, NT, preferred_element_type=F32) - shift
            m_old = m_ref[g, rows, :]
            m_new = jnp.maximum(m_old, jnp.max(s, axis=1, keepdims=True))
            p = jnp.exp(s - m_new[:, 0:1]).astype(BF)
            pv = jnp.dot(p, values, preferred_element_type=F32)
            acc_ref[g, rows, :] = acc_ref[g, rows, :] * jnp.exp(m_old - m_new) + pv
            m_ref[g, rows, :] = m_new
            return 0

        lax.fori_loop(0, 4, some, 0)

    if first:

        def start(g, _):
            diagonal(g)
            return 0

        lax.fori_loop(0, 4, start, 0)

    steps = (6, 16, 8)[call]

    def body(i, _):
        for u in range(UNROLL[call]):
            fast(UNROLL[call] * i + u)
        return 0

    lax.fori_loop(0, steps // UNROLL[call], body, 0)

    def look(g, bad):
        lane = lax.broadcasted_iota(jnp.int32, (ROWS_STEP, 128), 1)
        return bad + jnp.where((acc_ref[g] <= HUGE) | (lane > 0), 0.0, 1.0)

    bad = lax.fori_loop(0, 4, look, jnp.zeros((ROWS_STEP, 128), F32))

    @pl.when(jnp.max(bad) > 0.0)
    def _():
        if first:

            def restart(g, _):
                diagonal(g)
                return 0

            lax.fori_loop(0, 4, restart, 0)
        else:

            def restore(g, _):
                acc_ref[g] = acc_in[g]
                m_ref[g] = m_in[g]
                return 0

            lax.fori_loop(0, 4, restore, 0)

        def again(t, _):
            careful(t)
            return 0

        lax.fori_loop(0, steps, again, 0)

    if last:

        def finish(g, _):
            zq = table[0, 4 + g]
            lane = lax.broadcasted_iota(jnp.int32, (QG, 128), 1)
            for half, ref in ((core, keep_ref), (1 - core, send_ref)):
                rows = pl.ds(pl.multiple_of(half * QG, QG), QG)
                ref[zq] = jnp.where(lane == 0, m_ref[g, rows, :], acc_ref[g, rows, :])
            return 0

        lax.fori_loop(0, 4, finish, 0)


def attend(call, table, shared, kvs, state=None):
    n = CALLS[call]
    first, last = call == 0, call == 2
    vmem = pl.BlockSpec(memory_space=pltpu.VMEM)
    hbm = pl.BlockSpec(memory_space=pl.ANY)
    args = [table, *shared] + list(state or ()) + list(kvs)
    specs = [pl.BlockSpec(memory_space=pltpu.SMEM)] + [vmem] * (len(args) - 1 - n) + [hbm] * n
    pair = (4, ROWS_STEP, 128)
    if last:
        out_shape = [jax.ShapeDtypeStruct((4, QG, 128), F32)] * 2
    else:
        out_shape = [pltpu.VMEM(pair, F32)] * 2
    if first:
        out_shape = [pltpu.VMEM((128, 128), F32), pltpu.VMEM(pair, BF)] + out_shape
    scratch = [pltpu.VMEM((2048 * n, 128), BF), pltpu.SemaphoreType.DMA((n,))]
    if last:
        scratch += [pltpu.VMEM(pair, F32), pltpu.VMEM(pair, F32)]
    steps = (9, 16, 8)[call]
    return pl.pallas_call(
        functools.partial(attend_kernel, call, first, last),
        in_specs=specs,
        out_shape=out_shape,
        out_specs=[vmem] * len(out_shape),
        scratch_shapes=scratch,
        cost_estimate=pl.CostEstimate(
            flops=steps * ROWS_STEP * QG * 512 * 2,
            transcendentals=steps * ROWS_STEP * QG,
            bytes_accessed=n * 2048 * 256,
        ),
        name="attend",
        compiler_params=pltpu.CompilerParams(vmem_limit_bytes=14 * 2**20),
    )(*args)


def merge_kernel(keep, other, out_ref):
    lane64 = lax.broadcasted_iota(jnp.int32, (64, 128), 1) < 64
    for zq in range(4):
        for i in range(4):
            rows = slice(i * TILE, (i + 1) * TILE)
            a, b = keep[zq, rows, :], other[zq, rows, :]
            whole = (TILE, 128)
            m_a, m_b = jnp.broadcast_to(a[:, 0:1], whole), jnp.broadcast_to(b[:, 0:1], whole)
            l_a, l_b = jnp.broadcast_to(a[:, 1:2], whole), jnp.broadcast_to(b[:, 1:2], whole)
            w_a, w_b = jnp.exp(jnp.minimum(m_a - m_b, 0.0)), jnp.exp(jnp.minimum(m_b - m_a, 0.0))
            o = (a * w_a + b * w_b) * (1.0 / (l_a * w_a + l_b * w_b))
            packed = jnp.where(lane64, pltpu.roll(o[0:64], 64, 1), o[64:128])
            out_ref[zq * 4 + i, :, :] = packed.astype(BF)


def merge(keep, other):
    vmem = pl.BlockSpec(memory_space=pltpu.VMEM)
    return pl.pallas_call(
        merge_kernel,
        in_specs=[vmem, vmem],
        out_shape=pltpu.VMEM((16, 64, 128), BF),
        out_specs=vmem,
        name="merge",
        compiler_params=pltpu.CompilerParams(vmem_limit_bytes=12 * 2**20),
    )(keep, other)


def rms_scale(rows, gain):
    mean_sq = jnp.mean(rows * rows, axis=-1, keepdims=True)
    return rows * lax.rsqrt(mean_sq + NORM_EPS) * gain


PITCH = 24


def slots_of(ids):
    expert = lax.broadcasted_iota(jnp.int32, (TILE, 128), 1)
    first = (ids[:, 0:1] == expert).astype(F32)
    second = (ids[:, 1:2] == expert).astype(F32)
    named = first + second
    r = lax.broadcasted_iota(jnp.int32, (TILE, TILE), 0)
    c = lax.broadcasted_iota(jnp.int32, (TILE, TILE), 1)
    before = jnp.where(c < r, 1.0, 0.0).astype(BF)
    rank = jnp.dot(before, named.astype(BF), preferred_element_type=F32)
    return first, second, named, rank


def mix_kernel(
    got, w_hbm, residual, gain_mix, gain_pre, ids, stream, outgoing, x, proj, normed, scr, w_out, sems
):
    copies = [
        pltpu.make_async_copy(w_hbm.at[pl.ds(i * 256, 256)], w_out.at[pl.ds(i * 256, 256)], sems.at[i])
        for i in range(4)
    ]
    for c in copies:
        c.start()
    lane = lax.broadcasted_iota(jnp.int32, (64, 128), 1) < 64
    for hp in range(8):
        even, odd = 2 * hp, 2 * hp + 1

        def block(h):
            return got[(h % 4) * 4 + h // 4].astype(F32)

        e, o = block(even), block(odd)
        cols = slice(hp * 128, hp * 128 + 128)
        x[0:64, cols] = jnp.where(lane, e, pltpu.roll(o, 64, 1)).astype(BF)
        x[64:128, cols] = jnp.where(lane, pltpu.roll(e, 64, 1), o).astype(BF)
    for i, c in enumerate(copies):
        c.wait()
        k = slice(i * 256, i * 256 + 256)
        part = jnp.dot(x[:, k], w_out[k, :], preferred_element_type=F32)
        proj[...] = part if i == 0 else proj[...] + part

    def norm(i, _):
        rows = pl.ds(pl.multiple_of(i * 16, 16), 16)
        mixed = residual[rows, :].astype(F32) + rms_scale(proj[rows, :], gain_mix[...])
        rounded = mixed.astype(BF)
        stream[rows, :] = rounded
        normed[rows, :] = rms_scale(rounded.astype(F32), gain_pre[...]).astype(BF)
        return 0

    lax.fori_loop(0, 8, norm, 0)

    _, _, named, rank = slots_of(ids[...])
    tn = (((0,), (0,)), ((), ()))
    for s in range(3):
        sel = jnp.where(rank == s, named, 0.0).astype(BF)
        for j in range(0, 16, 2):
            part = normed[:, j * 128 : j * 128 + 256]
            res = lax.dot_general(sel, part, tn, preferred_element_type=F32)
            scr[pl.ds(s * 128 * PITCH + j, 128, stride=PITCH), :] = res[:, 0:128]
            scr[pl.ds(s * 128 * PITCH + j + 1, 128, stride=PITCH), :] = res[:, 128:256]

    def put(e, _):
        for s in range(3):
            src = pl.multiple_of((s * 128 + e) * PITCH, 8)
            dst = pl.multiple_of(e * 48 + s * 16, 16)
            outgoing[pl.ds(dst, 16), :] = scr[pl.ds(src, 16), :].astype(BF)
        return 0

    lax.fori_loop(0, 128, put, 0, unroll=4)


def mix(got, w_out, residual, gain_mix, gain_pre, ids):
    vmem = pl.BlockSpec(memory_space=pltpu.VMEM)
    return pl.pallas_call(
        mix_kernel,
        in_specs=[vmem, pl.BlockSpec(memory_space=pltpu.HBM)] + [vmem] * 4,
        out_shape=[pltpu.VMEM((TILE, 2048), BF), pltpu.VMEM((6144, 128), BF)],
        out_specs=[vmem, vmem],
        scratch_shapes=[
            pltpu.VMEM((TILE, 1024), BF),
            pltpu.VMEM((TILE, 2048), F32),
            pltpu.VMEM((TILE, 2048), BF),
            pltpu.VMEM((384 * PITCH, 128), F32),
            pltpu.VMEM((1024, 2048), BF),
            pltpu.SemaphoreType.DMA((4,)),
        ],
        name="mix",
        compiler_params=pltpu.CompilerParams(vmem_limit_bytes=14 * 2**20),
    )(got, pltpu.with_memory_space_constraint(w_out, pltpu.HBM), residual, gain_mix.reshape(1, -1), gain_pre.reshape(1, -1), ids)


def expert_kernel(arrived, w_gate, w_up, w_down, out, scr, x):
    def take(r, _):
        src = pl.multiple_of(r * 16, 16)
        scr[pl.ds(pl.multiple_of(r * PITCH, 8), 16), :] = arrived[pl.ds(src, 16), :].astype(F32)
        return 0

    lax.fori_loop(0, 384, take, 0, unroll=8)
    for j in range(16):
        x[:, j * 128 : j * 128 + 128] = scr[pl.ds(j, 384, stride=PITCH), :].astype(BF)
    gate_act = jnp.dot(x[...], w_gate[0], preferred_element_type=F32)
    up_act = jnp.dot(x[...], w_up[0], preferred_element_type=F32)
    hidden = (jax.nn.silu(gate_act) * up_act).astype(BF)
    for j in range(0, 16, 2):
        res = jnp.dot(hidden, w_down[0, :, j * 128 : j * 128 + 256], preferred_element_type=F32)
        scr[pl.ds(j, 384, stride=PITCH), :] = res[:, 0:128]
        scr[pl.ds(j + 1, 384, stride=PITCH), :] = res[:, 128:256]

    def put(r, _):
        dst = pl.multiple_of(r * 16, 16)
        out[pl.ds(dst, 16), :] = scr[pl.ds(pl.multiple_of(r * PITCH, 8), 16), :].astype(BF)
        return 0

    lax.fori_loop(0, 384, put, 0, unroll=8)


def expert(arrived, w_gate, w_up, w_down):
    vmem = pl.BlockSpec(memory_space=pltpu.VMEM)
    return pl.pallas_call(
        expert_kernel,
        in_specs=[vmem] * 4,
        out_shape=pltpu.VMEM((6144, 128), BF),
        out_specs=vmem,
        scratch_shapes=[pltpu.VMEM((384 * PITCH, 128), F32), pltpu.VMEM((384, 2048), BF)],
        name="expert",
        compiler_params=pltpu.CompilerParams(vmem_limit_bytes=18 * 2**20),
    )(arrived, w_gate, w_up, w_down)


def combine_kernel(returned, stream, ids, weight, gain_post, out, scr, comb):
    def take(e, _):
        for s in range(3):
            src = pl.multiple_of(e * 48 + s * 16, 16)
            dst = pl.multiple_of((s * 128 + e) * PITCH, 8)
            scr[pl.ds(dst, 16), :] = returned[pl.ds(src, 16), :].astype(F32)
        return 0

    lax.fori_loop(0, 128, take, 0, unroll=4)
    first, second, _, rank = slots_of(ids[...])
    w = weight[...]
    share = first * w[:, 0:1] + second * w[:, 1:2]
    full = jnp.concatenate([jnp.where(rank == s, share, 0.0) for s in range(3)], axis=1)
    hi = full.astype(BF)
    rest = full - hi.astype(F32)
    mid = rest.astype(BF)
    low = (rest - mid.astype(F32)).astype(BF)
    for j in range(16):
        rows = scr[pl.ds(j, 384, stride=PITCH), :].astype(BF)
        res = jnp.dot(low, rows, preferred_element_type=F32)
        res += jnp.dot(mid, rows, preferred_element_type=F32)
        res += jnp.dot(hi, rows, preferred_element_type=F32)
        comb[:, j * 128 : j * 128 + 128] = res

    def norm(i, _):
        rows = pl.ds(pl.multiple_of(i * 16, 16), 16)
        out[rows, :] = (stream[rows, :].astype(F32) + rms_scale(comb[rows, :], gain_post[...])).astype(BF)
        return 0

    lax.fori_loop(0, 8, norm, 0)


def combine(returned, stream, ids, weight, gain_post):
    vmem = pl.BlockSpec(memory_space=pltpu.VMEM)
    return pl.pallas_call(
        combine_kernel,
        in_specs=[vmem] * 5,
        out_shape=jax.ShapeDtypeStruct((TILE, 2048), BF),
        out_specs=vmem,
        scratch_shapes=[pltpu.VMEM((384 * PITCH, 128), F32), pltpu.VMEM((TILE, 2048), F32)],
        name="combine",
        compiler_params=pltpu.CompilerParams(vmem_limit_bytes=16 * 2**20),
    )(returned, stream, ids, weight, gain_post.reshape(1, -1))


def attention(queries, key_rows, value_rows, cum_gate):
    device = lax.axis_index("sp") * 8 + lax.axis_index("tp")
    table = lax.dynamic_slice_in_dim(jnp.asarray(device_table()), device, 1, 0)
    gate_own = cum_gate.reshape(256, 128)
    gate_peer = lax.ppermute(gate_own, "tp", CORE_PAIRS)
    msgs = pack(queries, key_rows, value_rows)
    recv = [
        lax.ppermute(msgs[2 * m1 + m2], ALL, exchange_pairs(m1, m2))
        for m1 in range(2)
        for m2 in range(2)
    ]
    own = jnp.concatenate([r[:QG] for r in recv], axis=0)
    from_left = lax.ppermute(own, "sp", ring_pairs(1))
    from_right = lax.ppermute(own, "sp", ring_pairs(-1))
    far_a = lax.ppermute(from_left[:1024], "sp", ring_pairs(1))
    far_b = lax.ppermute(from_right[1024:], "sp", ring_pairs(-1))
    gate, q_pad, *state = attend(0, table, (gate_own, gate_peer, *recv), [own])
    state = attend(1, table, (gate, q_pad), [from_left, from_right], state)
    far_own = jnp.concatenate([far_a, far_b], axis=0)
    keep, send = attend(2, table, (gate, q_pad), [far_own], state)
    out = merge(keep, lax.ppermute(send, "tp", CORE_PAIRS))
    return lax.all_to_all(out, ALL, split_axis=0, concat_axis=0, tiled=True, axis_index_groups=out_groups())


def local(
    queries,
    key_rows,
    value_rows,
    cum_gate,
    residual,
    out_weight,
    gain_mix,
    gain_pre,
    gain_post,
    route_ids,
    route_weight,
    w_gate,
    w_up,
    w_down,
):
    got = attention(queries, key_rows, value_rows, cum_gate)

    def exchange(rows):
        moved = lax.all_to_all(rows.reshape(128, 48, 128), ALL, split_axis=0, concat_axis=0, tiled=True)
        return moved.reshape(6144, 128)

    stream, outgoing = mix(got, out_weight, residual, gain_mix, gain_pre, route_ids)
    arrived = exchange(outgoing)
    returned = exchange(expert(arrived, w_gate, w_up, w_down))
    return combine(returned, stream, route_ids, route_weight, gain_post)


def solution(mesh):
    return jax.shard_map(
        local,
        mesh=mesh,
        in_specs=(
            P("sp", "tp"),
            P("sp", "tp"),
            P("sp", "tp"),
            P("tp", None),
            P(("sp", "tp"), None),
            P(),
            P(),
            P(),
            P(),
            P(("sp", "tp"), None),
            P(("sp", "tp"), None),
            P(("sp", "tp"), None, None),
            P(("sp", "tp"), None, None),
            P(("sp", "tp"), None, None),
        ),
        out_specs=P(("sp", "tp"), None),
        check_vma=False,
    )
```

```python
import functools

import jax
import jax.numpy as jnp
import numpy as np
from jax import lax
from jax.experimental import pallas as pl
from jax.experimental.pallas import tpu as pltpu
from jax.sharding import PartitionSpec as P

HEAD_DIM = 64
NORM_EPS = 1e-06
MASKED = -1e30
BF = jnp.bfloat16
F32 = jnp.float32
ALL = ("sp", "tp")
BLK = 1024
TILE = 128
QG = 512


def member(k, z):
    return 4 * z + (k if z % 2 == 0 else 3 - k)


def group_of(sp):
    z, x = divmod(sp, 4)
    return x if z % 2 == 0 else 3 - x


def exchange_pairs(m1, m2):
    pairs = []
    for sp in range(16):
        z = sp // 4
        for tp in range(8):
            y, s = divmod(tp, 2)
            to_z = 2 * s + (m1 ^ (z & 1))
            to_c = m2 ^ (z >> 1)
            pairs.append((sp * 8 + tp, member(group_of(sp), to_z) * 8 + 2 * y + to_c))
    return pairs


def ring_pairs(step):
    return [(sp, 4 * (sp // 4) + (sp % 4 + step) % 4) for sp in range(16)]


def out_groups():
    return [
        [member(k, z) * 8 + 2 * y + c for z in range(4) for y in range(4)]
        for k in range(4)
        for c in range(2)
    ]


CORE_PAIRS = [(i, i ^ 1) for i in range(8)]


def pack_kernel(q_in, k_in, v_in, *refs):
    outs, (q_ref, k_ref, v_ref, sems) = refs[:4], refs[4:]
    copies = [
        pltpu.make_async_copy(src, dst, sems.at[i])
        for i, (src, dst) in enumerate(((q_in, q_ref), (k_in, k_ref), (v_in, v_ref)))
    ]
    for c in copies:
        c.start()
    z = lax.axis_index("sp") // 4
    row = lax.broadcasted_iota(jnp.int32, (128, 128), 0)
    col = lax.broadcasted_iota(jnp.int32, (128, 128), 1)

    def dot(a, b):
        return jnp.dot(a, b, preferred_element_type=F32)

    for c in copies:
        c.wait()
    for m1 in range(2):
        f1 = m1 ^ (z & 1)
        low = jnp.where((col < 64) & (row == col + 64 * f1), 1.0, 0.0)
        high = jnp.where((col >= 64) & (row == col - 64 + 64 * f1), 1.0, 0.0)
        sel_lo, sel_hi = low.astype(BF), high.astype(BF)
        q_lo, q_hi = (low * 0.125).astype(BF), (high * 0.125).astype(BF)
        for i in range(4):
            even = q_ref[2 * i * TILE : (2 * i + 1) * TILE, :]
            odd = q_ref[(2 * i + 1) * TILE : (2 * i + 2) * TILE, :]
            qq = (dot(even, q_lo) + dot(odd, q_hi)).astype(BF)
            for m2 in range(2):
                outs[2 * m1 + m2][QG + i * TILE : QG + (i + 1) * TILE, :] = qq
        for m2 in range(2):
            f2 = m2 ^ (z >> 1)
            out = outs[2 * m1 + m2]
            for i in range(4):
                src = pl.ds(pl.multiple_of((2 * i + f2) * TILE, TILE), TILE)
                kv = dot(k_ref[src, :], sel_lo) + dot(v_ref[src, :], sel_hi)
                out[i * TILE : (i + 1) * TILE, :] = kv.astype(BF)


def pack(q, k, v):
    return pl.pallas_call(
        pack_kernel,
        in_specs=[pl.BlockSpec(memory_space=pltpu.HBM)] * 3,
        out_shape=[pltpu.VMEM((BLK, 128), BF)] * 4,
        out_specs=[pl.BlockSpec(memory_space=pltpu.VMEM)] * 4,
        scratch_shapes=[pltpu.VMEM((BLK, 128), BF)] * 3 + [pltpu.SemaphoreType.DMA((3,))],
        name="pack",
        compiler_params=pltpu.CompilerParams(vmem_limit_bytes=8 * 2**20),
    )(*(pltpu.with_memory_space_constraint(a, pltpu.HBM) for a in (q, k, v)))


ROWS_STEP = 1024
FR, FK, AHEAD = 512, 256, 1
UNROLL = (3, 4, 4)
HUGE = 1e30
CALLS = (1, 2, 1)
STEP0 = (16, 72, 144)


def block_of(z, core, slot, x_of):
    zb = ((slot // 2) ^ (z & 1)) + 2 * ((slot % 2) ^ core)
    return zb, 4 * zb + (3 - x_of if slot // 2 else x_of)


def device_table():
    table = np.zeros((128, 256), np.int32)
    for sp in range(16):
        z, x = divmod(sp, 4)
        for core in range(2):
            row = np.zeros(256, np.int32)
            row[0:3] = z, x, core
            zq = [block_of(z, core, g, x)[0] for g in range(4)]
            row[4:8] = zq
            for call, chunks in enumerate(((x,), ((x + 3) % 4, (x + 1) % 4), ((x + 2) % 4,))):
                steps = []
                for i, x_of in enumerate(chunks):
                    for g in range(4):
                        for slot in range(4):
                            b_q, b_k = block_of(z, core, g, x)[1], block_of(z, core, slot, x_of)[1]
                            if b_k < b_q:
                                steps.append((g, i * 2048 + slot * QG, b_k * 8, b_q * 8))
                assert len(steps) == (6, 16, 8)[call]
                flat = np.array(steps + [(0, 0, 0, 0)] * 2, np.int32).reshape(-1)
                row[STEP0[call] : STEP0[call] + len(flat)] = flat
            for y in range(4):
                table[sp * 8 + 2 * y + core] = row
    return table


NT = (((1,), (1,)), ((), ()))


def attend_kernel(call, first, last, table, *refs):
    refs = list(refs)
    n = CALLS[call]
    if first:
        gate_own, gate_peer = refs.pop(0), refs.pop(0)
        qs = [refs.pop(0) for _ in range(4)]
    else:
        gate, q_pad, m_in, acc_in = [refs.pop(0) for _ in range(4)]
    kv_in = [refs.pop(0) for _ in range(n)]
    if first:
        gate, q_pad, m_ref, acc_ref = [refs.pop(0) for _ in range(4)]
    elif last:
        w_hbm = refs.pop(0)
        keep_ref, send_ref, w_ref = [refs.pop(0) for _ in range(3)]
    else:
        m_ref, acc_ref = refs.pop(0), refs.pop(0)
    kv, sems = refs.pop(0), refs.pop(0)
    if last:
        m_ref, acc_ref, w_sem = [refs.pop(0) for _ in range(3)]
    z, core = table[0, 0], table[0, 2]

    copies = [pltpu.make_async_copy(src, kv.at[pl.ds(i * 2048, 2048)], sems.at[i]) for i, src in enumerate(kv_in)]
    for c in copies:
        c.start()
    if last:
        w_copy = pltpu.make_async_copy(w_hbm, w_ref, w_sem)
        w_copy.start()
    if first:
        mine = lax.shift_right_logical(z, 1) == core
        row0 = pl.multiple_of((z & 1) * 128, 128)
        gate[...] = jnp.where(mine, gate_own[pl.ds(row0, 128), :], gate_peer[pl.ds(row0, 128), :])
        lane = lax.broadcasted_iota(jnp.int32, (QG, 128), 1)
        for g in range(4):
            packed = qs[g][QG:, :].astype(F32)
            q_pad[g, 0:QG, :] = jnp.where(lane < 64, packed, 0.0).astype(BF)
            q_pad[g, QG:, :] = jnp.where(lane < 64, pltpu.roll(packed, 64, 1), 0.0).astype(BF)
    else:
        acc_ref[...] = acc_in[...]
        m_ref[...] = m_in[...]
    for c in copies:
        c.wait()

    def operands(start, key_gate, query_gate):
        keys = kv[pl.ds(pl.multiple_of(start, QG), QG), :]
        parts = [gate[pl.ds(key_gate + 2 * i + core, 1), :] for i in range(4)]
        shift = jnp.concatenate(parts, axis=1) - gate[pl.ds(query_gate, 1), 0:1]
        ones = lax.broadcasted_iota(jnp.int32, (QG, 128), 1) < 64
        return keys, jnp.where(ones, jnp.ones_like(keys), keys), shift

    def spread(rows):
        return jnp.concatenate([rows] * (FK // 128), axis=1)

    def diagonal(g):
        block = 4 * table[0, 4 + g] * 8 + xb_of(g) * 8
        keys, values, shift = operands(g * QG, block, block)
        r = lax.broadcasted_iota(jnp.int32, (TILE, TILE), 0)
        cc = lax.broadcasted_iota(jnp.int32, (TILE, TILE), 1)
        tri = jnp.where(cc <= r, 0.0, MASKED)
        even = jnp.where(core == 0, tri, jnp.full_like(tri, MASKED))
        odd = jnp.where(core == 0, jnp.zeros_like(tri), tri)
        edge = jnp.concatenate([even, odd], axis=0)
        for i in range(4):
            lo, hi = slice(i * TILE, (i + 1) * TILE), slice(QG + i * TILE, QG + (i + 1) * TILE)
            q = jnp.concatenate([q_pad[g, lo, :], q_pad[g, hi, :]], axis=0)
            width = (i + 1) * TILE
            s = lax.dot_general(q, keys[0:width], NT, preferred_element_type=F32) - shift[:, 0:width]
            raw = s[:, width - TILE :]
            s_edge = raw + edge
            top = jnp.max(s_edge, axis=1, keepdims=True)
            if i == 0:
                level = -4.0 * jnp.sum(jnp.abs(q.astype(F32)), axis=1, keepdims=True)
                top = jnp.where(top <= 0.1 * MASKED, level, top)
                p = jnp.exp(s_edge - top).astype(BF)
            else:
                body = s[:, 0 : width - TILE]
                top = jnp.maximum(top, jnp.max(body, axis=1, keepdims=True))
                p = jnp.exp(jnp.concatenate([body, s_edge], axis=1) - top).astype(BF)
            pv = jnp.dot(p, values[0:width], preferred_element_type=F32)
            top = jnp.broadcast_to(top, (2 * TILE, 128))
            acc_ref[g, lo, :], acc_ref[g, hi, :] = pv[0:TILE], pv[TILE:]
            m_ref[g, lo, :], m_ref[g, hi, :] = top[0:TILE], top[TILE:]

    def xb_of(g):
        return jnp.where(g // 2 == 1, 3 - table[0, 1], table[0, 1])

    def step_operands(t):
        at = STEP0[call] + 4 * t
        return table[0, at], operands(table[0, at + 1], table[0, at + 2], table[0, at + 3])

    def fast(t):
        g, (keys, values, shift) = step_operands(t)
        units = [(r0, k0) for r0 in range(0, ROWS_STEP, FR) for k0 in range(0, QG, FK)]

        def qk(r0, k0):
            return lax.dot_general(q_pad[g, r0 : r0 + FR, :], keys[k0 : k0 + FK], NT, preferred_element_type=F32)

        ahead = [qk(*units[i]) for i in range(AHEAD)]
        pv = None
        for u, (r0, k0) in enumerate(units):
            s = ahead.pop(0)
            if u + AHEAD < len(units):
                ahead.append(qk(*units[u + AHEAD]))
            m_rows = spread(m_ref[g, r0 : r0 + FR, :])
            p = jnp.exp(s - shift[:, k0 : k0 + FK] - m_rows).astype(BF)
            part = jnp.dot(p, values[k0 : k0 + FK], preferred_element_type=F32)
            pv = part if k0 == 0 else pv + part
            if k0 + FK == QG:
                acc_ref[g, r0 : r0 + FR, :] += pv

    def careful(t):
        g, (keys, values, shift) = step_operands(t)

        def some(i, _):
            rows = pl.ds(pl.multiple_of(i * 256, 256), 256)
            s = lax.dot_general(q_pad[g, rows, :], keys, NT, preferred_element_type=F32) - shift
            m_old = m_ref[g, rows, :]
            m_new = jnp.maximum(m_old, jnp.max(s, axis=1, keepdims=True))
            p = jnp.exp(s - m_new[:, 0:1]).astype(BF)
            pv = jnp.dot(p, values, preferred_element_type=F32)
            acc_ref[g, rows, :] = acc_ref[g, rows, :] * jnp.exp(m_old - m_new) + pv
            m_ref[g, rows, :] = m_new
            return 0

        lax.fori_loop(0, 4, some, 0)

    if first:

        def start(g, _):
            diagonal(g)
            return 0

        lax.fori_loop(0, 4, start, 0)

    steps = (6, 16, 8)[call]

    def body(i, _):
        for u in range(UNROLL[call]):
            fast(UNROLL[call] * i + u)
        return 0

    lax.fori_loop(0, steps // UNROLL[call], body, 0)

    def look(g, bad):
        lane = lax.broadcasted_iota(jnp.int32, (ROWS_STEP, 128), 1)
        return bad + jnp.where((acc_ref[g] <= HUGE) | (lane > 0), 0.0, 1.0)

    bad = lax.fori_loop(0, 4, look, jnp.zeros((ROWS_STEP, 128), F32))

    @pl.when(jnp.max(bad) > 0.0)
    def _():
        if first:

            def restart(g, _):
                diagonal(g)
                return 0

            lax.fori_loop(0, 4, restart, 0)
        else:

            def restore(g, _):
                acc_ref[g] = acc_in[g]
                m_ref[g] = m_in[g]
                return 0

            lax.fori_loop(0, 4, restore, 0)

        def again(t, _):
            careful(t)
            return 0

        lax.fori_loop(0, steps, again, 0)

    if last:

        def finish(g, _):
            zq = table[0, 4 + g]
            lane = lax.broadcasted_iota(jnp.int32, (QG, 128), 1)
            for half, ref in ((core, keep_ref), (1 - core, send_ref)):
                rows = pl.ds(pl.multiple_of(half * QG, QG), QG)
                ref[zq] = jnp.where(lane == 0, m_ref[g, rows, :], acc_ref[g, rows, :])
            return 0

        lax.fori_loop(0, 4, finish, 0)
        w_copy.wait()


def attend(call, table, shared, kvs, state=None, w_out=None):
    n = CALLS[call]
    first, last = call == 0, call == 2
    vmem = pl.BlockSpec(memory_space=pltpu.VMEM)
    hbm = pl.BlockSpec(memory_space=pl.ANY)
    args = [table, *shared] + list(state or ()) + list(kvs)
    specs = [pl.BlockSpec(memory_space=pltpu.SMEM)] + [vmem] * (len(args) - 1 - n) + [hbm] * n
    pair = (4, ROWS_STEP, 128)
    if last:
        args.append(pltpu.with_memory_space_constraint(w_out, pltpu.HBM))
        specs.append(pl.BlockSpec(memory_space=pltpu.HBM))
        out_shape = [jax.ShapeDtypeStruct((4, QG, 128), F32)] * 2 + [pltpu.VMEM(w_out.shape, BF)]
    else:
        out_shape = [pltpu.VMEM(pair, F32)] * 2
    if first:
        out_shape = [pltpu.VMEM((128, 128), F32), pltpu.VMEM(pair, BF)] + out_shape
    scratch = [pltpu.VMEM((2048 * n, 128), BF), pltpu.SemaphoreType.DMA((n,))]
    if last:
        scratch += [pltpu.VMEM(pair, F32), pltpu.VMEM(pair, F32), pltpu.SemaphoreType.DMA]
    steps = (9, 16, 8)[call]
    return pl.pallas_call(
        functools.partial(attend_kernel, call, first, last),
        in_specs=specs,
        out_shape=out_shape,
        out_specs=[vmem] * len(out_shape),
        scratch_shapes=scratch,
        cost_estimate=pl.CostEstimate(
            flops=steps * ROWS_STEP * QG * 512 * 2,
            transcendentals=steps * ROWS_STEP * QG,
            bytes_accessed=n * 2048 * 256,
        ),
        name="attend",
        compiler_params=pltpu.CompilerParams(vmem_limit_bytes=14 * 2**20),
    )(*args)


def merge_kernel(keep, other, out_ref):
    lane64 = lax.broadcasted_iota(jnp.int32, (64, 128), 1) < 64
    for zq in range(4):
        for i in range(4):
            rows = slice(i * TILE, (i + 1) * TILE)
            a, b = keep[zq, rows, :], other[zq, rows, :]
            whole = (TILE, 128)
            m_a, m_b = jnp.broadcast_to(a[:, 0:1], whole), jnp.broadcast_to(b[:, 0:1], whole)
            l_a, l_b = jnp.broadcast_to(a[:, 1:2], whole), jnp.broadcast_to(b[:, 1:2], whole)
            w_a, w_b = jnp.exp(jnp.minimum(m_a - m_b, 0.0)), jnp.exp(jnp.minimum(m_b - m_a, 0.0))
            o = (a * w_a + b * w_b) * (1.0 / (l_a * w_a + l_b * w_b))
            packed = jnp.where(lane64, pltpu.roll(o[0:64], 64, 1), o[64:128])
            out_ref[zq * 4 + i, :, :] = packed.astype(BF)


def merge(keep, other):
    vmem = pl.BlockSpec(memory_space=pltpu.VMEM)
    return pl.pallas_call(
        merge_kernel,
        in_specs=[vmem, vmem],
        out_shape=pltpu.VMEM((16, 64, 128), BF),
        out_specs=vmem,
        name="merge",
        compiler_params=pltpu.CompilerParams(vmem_limit_bytes=12 * 2**20),
    )(keep, other)


def rms_scale(rows, gain):
    mean_sq = jnp.mean(rows * rows, axis=-1, keepdims=True)
    return rows * lax.rsqrt(mean_sq + NORM_EPS) * gain


PITCH = 24


def column(row):
    return jnp.transpose(jnp.broadcast_to(row, (TILE, 128)))


def slots_of(ids):
    expert = lax.broadcasted_iota(jnp.int32, (TILE, 128), 1)
    first = (column(ids[0:1, :]) == expert).astype(F32)
    second = (column(ids[1:2, :]) == expert).astype(F32)
    named = first + second
    r = lax.broadcasted_iota(jnp.int32, (TILE, TILE), 0)
    c = lax.broadcasted_iota(jnp.int32, (TILE, TILE), 1)
    before = jnp.where(c < r, 1.0, 0.0).astype(BF)
    rank = jnp.dot(before, named.astype(BF), preferred_element_type=F32)
    return first, second, named, rank


def mix_kernel(
    got, w_out, residual, gain_mix, gain_pre, ids, stream, outgoing, x, proj, normed, scr
):
    lane = lax.broadcasted_iota(jnp.int32, (64, 128), 1) < 64
    for hp in range(8):
        even, odd = 2 * hp, 2 * hp + 1

        def block(h):
            return got[(h % 4) * 4 + h // 4].astype(F32)

        e, o = block(even), block(odd)
        cols = slice(hp * 128, hp * 128 + 128)
        x[0:64, cols] = jnp.where(lane, e, pltpu.roll(o, 64, 1)).astype(BF)
        x[64:128, cols] = jnp.where(lane, pltpu.roll(e, 64, 1), o).astype(BF)
    proj[...] = jnp.dot(x[...], w_out[...], preferred_element_type=F32)

    def norm(i, _):
        rows = pl.ds(pl.multiple_of(i * 16, 16), 16)
        mixed = residual[rows, :].astype(F32) + rms_scale(proj[rows, :], gain_mix[...])
        rounded = mixed.astype(BF)
        stream[rows, :] = rounded
        normed[rows, :] = rms_scale(rounded.astype(F32), gain_pre[...]).astype(BF)
        return 0

    lax.fori_loop(0, 8, norm, 0)

    _, _, named, rank = slots_of(ids[...])
    tn = (((0,), (0,)), ((), ()))
    for s in range(3):
        sel = jnp.where(rank == s, named, 0.0).astype(BF)
        for j in range(0, 16, 2):
            part = normed[:, j * 128 : j * 128 + 256]
            res = lax.dot_general(sel, part, tn, preferred_element_type=F32)
            scr[pl.ds(s * 128 * PITCH + j, 128, stride=PITCH), :] = res[:, 0:128]
            scr[pl.ds(s * 128 * PITCH + j + 1, 128, stride=PITCH), :] = res[:, 128:256]

    def put(e, _):
        for s in range(3):
            src = pl.multiple_of((s * 128 + e) * PITCH, 8)
            dst = pl.multiple_of(e * 48 + s * 16, 16)
            outgoing[pl.ds(dst, 16), :] = scr[pl.ds(src, 16), :].astype(BF)
        return 0

    lax.fori_loop(0, 128, put, 0, unroll=4)


def mix(got, w_out, residual, gain_mix, gain_pre, ids):
    vmem = pl.BlockSpec(memory_space=pltpu.VMEM)
    return pl.pallas_call(
        mix_kernel,
        in_specs=[vmem] * 6,
        out_shape=[pltpu.VMEM((TILE, 2048), BF), pltpu.VMEM((6144, 128), BF)],
        out_specs=[vmem, vmem],
        scratch_shapes=[
            pltpu.VMEM((TILE, 1024), BF),
            pltpu.VMEM((TILE, 2048), F32),
            pltpu.VMEM((TILE, 2048), BF),
            pltpu.VMEM((384 * PITCH, 128), F32),
        ],
        name="mix",
        compiler_params=pltpu.CompilerParams(vmem_limit_bytes=14 * 2**20),
    )(got, w_out, residual, gain_mix.reshape(1, -1), gain_pre.reshape(1, -1), ids)


def expert_kernel(arrived, w_gate, w_up, w_down, out, scr, x):
    def take(r, _):
        src = pl.multiple_of(r * 16, 16)
        scr[pl.ds(pl.multiple_of(r * PITCH, 8), 16), :] = arrived[pl.ds(src, 16), :].astype(F32)
        return 0

    lax.fori_loop(0, 384, take, 0, unroll=8)
    for j in range(16):
        x[:, j * 128 : j * 128 + 128] = scr[pl.ds(j, 384, stride=PITCH), :].astype(BF)
    gate_act = jnp.dot(x[...], w_gate[0], preferred_element_type=F32)
    up_act = jnp.dot(x[...], w_up[0], preferred_element_type=F32)
    hidden = (jax.nn.silu(gate_act) * up_act).astype(BF)
    for j in range(0, 16, 2):
        res = jnp.dot(hidden, w_down[0, :, j * 128 : j * 128 + 256], preferred_element_type=F32)
        scr[pl.ds(j, 384, stride=PITCH), :] = res[:, 0:128]
        scr[pl.ds(j + 1, 384, stride=PITCH), :] = res[:, 128:256]

    def put(r, _):
        dst = pl.multiple_of(r * 16, 16)
        out[pl.ds(dst, 16), :] = scr[pl.ds(pl.multiple_of(r * PITCH, 8), 16), :].astype(BF)
        return 0

    lax.fori_loop(0, 384, put, 0, unroll=8)


def expert(arrived, w_gate, w_up, w_down):
    vmem = pl.BlockSpec(memory_space=pltpu.VMEM)
    return pl.pallas_call(
        expert_kernel,
        in_specs=[vmem] * 4,
        out_shape=pltpu.VMEM((6144, 128), BF),
        out_specs=vmem,
        scratch_shapes=[pltpu.VMEM((384 * PITCH, 128), F32), pltpu.VMEM((384, 2048), BF)],
        name="expert",
        compiler_params=pltpu.CompilerParams(vmem_limit_bytes=18 * 2**20),
    )(arrived, w_gate, w_up, w_down)


def combine_kernel(returned, stream, ids, weight, gain_post, out, scr, comb):
    def take(e, _):
        for s in range(3):
            src = pl.multiple_of(e * 48 + s * 16, 16)
            dst = pl.multiple_of((s * 128 + e) * PITCH, 8)
            scr[pl.ds(dst, 16), :] = returned[pl.ds(src, 16), :].astype(F32)
        return 0

    lax.fori_loop(0, 128, take, 0, unroll=4)
    first, second, _, rank = slots_of(ids[...])
    w = weight[...]
    share = first * column(w[0:1, :]) + second * column(w[1:2, :])
    full = jnp.concatenate([jnp.where(rank == s, share, 0.0) for s in range(3)], axis=1)
    hi = full.astype(BF)
    rest = full - hi.astype(F32)
    mid = rest.astype(BF)
    low = (rest - mid.astype(F32)).astype(BF)
    for j in range(16):
        rows = scr[pl.ds(j, 384, stride=PITCH), :].astype(BF)
        res = jnp.dot(low, rows, preferred_element_type=F32)
        res += jnp.dot(mid, rows, preferred_element_type=F32)
        res += jnp.dot(hi, rows, preferred_element_type=F32)
        comb[:, j * 128 : j * 128 + 128] = res

    def norm(i, _):
        rows = pl.ds(pl.multiple_of(i * 16, 16), 16)
        out[rows, :] = (stream[rows, :].astype(F32) + rms_scale(comb[rows, :], gain_post[...])).astype(BF)
        return 0

    lax.fori_loop(0, 8, norm, 0)


def combine(returned, stream, ids, weight, gain_post):
    vmem = pl.BlockSpec(memory_space=pltpu.VMEM)
    return pl.pallas_call(
        combine_kernel,
        in_specs=[vmem] * 5,
        out_shape=jax.ShapeDtypeStruct((TILE, 2048), BF),
        out_specs=vmem,
        scratch_shapes=[pltpu.VMEM((384 * PITCH, 128), F32), pltpu.VMEM((TILE, 2048), F32)],
        name="combine",
        compiler_params=pltpu.CompilerParams(vmem_limit_bytes=16 * 2**20),
    )(returned, stream, ids, weight, gain_post.reshape(1, -1))


def attention(queries, key_rows, value_rows, cum_gate, out_weight):
    device = lax.axis_index("sp") * 8 + lax.axis_index("tp")
    table = lax.dynamic_slice_in_dim(jnp.asarray(device_table()), device, 1, 0)
    gate_own = cum_gate.reshape(256, 128)
    gate_peer = lax.ppermute(gate_own, "tp", CORE_PAIRS)
    msgs = pack(queries, key_rows, value_rows)
    recv = [
        lax.ppermute(msgs[2 * m1 + m2], ALL, exchange_pairs(m1, m2))
        for m1 in range(2)
        for m2 in range(2)
    ]
    own = jnp.concatenate([r[:QG] for r in recv], axis=0)
    from_left = lax.ppermute(own, "sp", ring_pairs(1))
    from_right = lax.ppermute(own, "sp", ring_pairs(-1))
    far_a = lax.ppermute(from_left[:1024], "sp", ring_pairs(1))
    far_b = lax.ppermute(from_right[1024:], "sp", ring_pairs(-1))
    gate, q_pad, *state = attend(0, table, (gate_own, gate_peer, *recv), [own])
    state = attend(1, table, (gate, q_pad), [from_left, from_right], state)
    far_own = jnp.concatenate([far_a, far_b], axis=0)
    keep, send, w_vmem = attend(2, table, (gate, q_pad), [far_own], state, out_weight)
    out = merge(keep, lax.ppermute(send, "tp", CORE_PAIRS))
    got = lax.all_to_all(out, ALL, split_axis=0, concat_axis=0, tiled=True, axis_index_groups=out_groups())
    return got, w_vmem


def local(
    queries,
    key_rows,
    value_rows,
    cum_gate,
    residual,
    out_weight,
    gain_mix,
    gain_pre,
    gain_post,
    route_ids,
    route_weight,
    w_gate,
    w_up,
    w_down,
):
    got, w_vmem = attention(queries, key_rows, value_rows, cum_gate, out_weight)

    def exchange(rows):
        moved = lax.all_to_all(rows.reshape(128, 48, 128), ALL, split_axis=0, concat_axis=0, tiled=True)
        return moved.reshape(6144, 128)

    stream, outgoing = mix(got, w_vmem, residual, gain_mix, gain_pre, route_ids.T)
    arrived = exchange(outgoing)
    returned = exchange(expert(arrived, w_gate, w_up, w_down))
    return combine(returned, stream, route_ids.T, route_weight.T, gain_post)


def solution(mesh):
    return jax.shard_map(
        local,
        mesh=mesh,
        in_specs=(
            P("sp", "tp"),
            P("sp", "tp"),
            P("sp", "tp"),
            P("tp", None),
            P(("sp", "tp"), None),
            P(),
            P(),
            P(),
            P(),
            P(("sp", "tp"), None),
            P(("sp", "tp"), None),
            P(("sp", "tp"), None, None),
            P(("sp", "tp"), None, None),
            P(("sp", "tp"), None, None),
        ),
        out_specs=P(("sp", "tp"), None),
        check_vma=False,
    )
```
